256 devices in a mesh: gr: 2 (over z_hi), fs: 16 (over z_lo, x), tp: 8 (over y, core).
Axes of the slice: x: 4, y: 4, z: 8 (z_hi: 2, z_lo: 4; z = z_hi * 4 + z_lo), core: 2. Of those that a mesh axis runs over, the one named last changes fastest.
Arguments:
- tokens: bfloat16 [16384, 2048], P(('gr', 'fs')), may hold values from -6 to 6
- routes: int32 [16384, 2], P(('gr', 'fs')), may hold values from 0 to 15, all different within a row; in each aligned block of 512 rows (0 to 511, 512 to 1023, ...) at most 96 rows name the same one
- route_weight: float32 [16384, 2], P(('gr', 'fs')), may hold values from 0.2 to 1
- gain: float32 [2048], P(('gr', 'fs')), may hold values from 0.1 to 1.9
- w_gate: bfloat16 [16, 2048, 4096], P(None, ('gr', 'fs'), 'tp'), may hold values from -0.125 to 0.125
- w_up: bfloat16 [16, 2048, 4096], P(None, ('gr', 'fs'), 'tp'), may hold values from -0.125 to 0.125
- w_down: bfloat16 [16, 2048, 4096], P(None, ('gr', 'fs'), 'tp'), may hold values from -0.09375 to 0.09375
Outputs:
- gate_out: bfloat16 [16, 2048, 4096], P('fs', None, 'tp')
- up_out: bfloat16 [16, 2048, 4096], P('fs', None, 'tp')
- down_out: bfloat16 [16, 2048, 4096], P('fs', None, 'tp')
- mixed: bfloat16 [16384, 2048], P(('gr', 'fs'), 'tp')
The draws below stay inside these ranges and needn't reach their ends.
Inputs may be any that keep to these rules, and one draw needn't show every extreme that they name: `routes`: each row names two different experts. Among the 512 rows of one device no expert is named more than 96 times, and in every draw some device names some expert exactly 96 times.
All inputs are finite; a program needn't handle non-finite values.
Results may differ from the reference program's by a relative error of at most 0.015.
Values may be sent and summed in bfloat16 or wider, within the bound.
A program may use at most 128 MiB of HBM per device.

```python
import math
import jax
import jax.numpy as jnp
import numpy as np
from jax import lax

D = 2048
FF = 4096
EXPERTS = 16
TOK_DEV = 512
CAP = 96
TOKENS = 16384
N_GR = 2
N_FS = 16
N_TP = 8


def level_of(rng, extent, cuts, low, largest):
    def one(position, shards_of):
        heights = jax.random.uniform(jax.random.fold_in(jax.random.fold_in(rng, 6), position), (shards_of,), jnp.float32, low / len(cuts), largest / len(cuts))
        return jnp.repeat(jnp.exp(heights), extent[position] // shards_of).reshape((-1,) + (1,) * (len(extent) - position - 1))

    factor_of = one(*cuts[0])
    for cut in cuts[1:]:
        factor_of = factor_of * one(*cut)
    return factor_of


def deal_out(own_key, own, number, rows, amount, top, bound, skew):
    order = jax.random.permutation(own_key, amount)
    heavy_load, ordinary = portions_of(amount, rows * top, bound, skew, True), portions_of(amount, rows * top, bound, skew, False)
    places = jnp.arange(amount)

    def named(tallies, rotation):
        used = int((tallies > 0).sum())
        fixed = max(1, used // 4)
        passed = fixed + (places - fixed + rotation * (used - fixed)) % max(1, amount - fixed)
        return jnp.zeros((amount,), jnp.int32).at[order[jnp.where(places < fixed, places, passed)]].set(jnp.asarray(tallies, jnp.int32))

    tallies = jnp.where(number % 4 == 0, named(heavy_load, number // 4), named(ordinary, number - number // 4 - 1))
    mixed = jax.random.permutation(jax.random.fold_in(own, 3), amount)
    donor, sink = mixed[0:amount // 2 * 2:2], mixed[1:amount // 2 * 2:2]
    margin = jnp.minimum(tallies[donor] - 1, bound - tallies[sink]) // 2
    margin = jnp.where((donor == order[0]) | (sink == order[0]) | (tallies[sink] == 0), 0, jnp.maximum(margin, 0))
    passed = jax.random.randint(jax.random.fold_in(own, 4), (amount // 2,), 0, 1 << 20) % (margin + 1)
    tallies = tallies.at[donor].add(-passed).at[sink].add(passed)
    members = jnp.searchsorted(jnp.cumsum(tallies), jnp.arange(rows * top), side="right").astype(jnp.int32)
    table = members.reshape(top, rows).T
    table = table[jax.random.permutation(jax.random.fold_in(own, 1), rows)]
    rotation = jax.random.randint(jax.random.fold_in(own, 2), (rows, 1), 0, top)
    return jnp.take_along_axis(table, (jnp.arange(top)[None, :] + rotation) % top, axis=1)


def portions_of(number_of, total, most, slope, full):
    portions = [(1 << 20) // math.isqrt(standing ** slope) + 1 for standing in range(1, number_of + 1)]
    largest = most if full else min(most, max(-(-total // number_of), total * portions[0] // sum(portions)))
    least = 1 if total - largest >= number_of - 1 else 0
    counts, spare = [largest] + [least] * (number_of - 1), total - largest - least * (number_of - 1)
    while spare > 0:
        candidates = [i for i in range(1, number_of) if counts[i] < largest] or [i for i in range(1, number_of) if counts[i] < most]
        pool, budget = sum([portions[i] for i in candidates]), spare
        for i in candidates:
            extra = min(most - counts[i], max(1, budget * portions[i] // pool), spare)
            counts[i] = counts[i] + extra
            spare = spare - extra
    return np.array(counts)


def gaussian(stream_key, shape, scale, most, shards=(), kind=jnp.bfloat16):
    level = level_of(stream_key, shape, shards, -0.22, 0.18) if shards else 1.0
    drawn = jax.random.normal(stream_key, shape, jnp.float32) * scale * level
    return jnp.minimum(jnp.maximum(drawn, -most), most).astype(kind)


def setup_inputs(seed: int = 0) -> dict:
    keys = jax.random.split(jax.random.key(seed), 8)
    tokens = gaussian(keys[0], (TOKENS, D), 1.0, 6.0, ((0, 32),))
    routes_keys = jax.random.split(jax.random.fold_in(keys[1], 1), TOKENS // TOK_DEV)
    routes_turns = jax.random.permutation(jax.random.fold_in(keys[1], 3), TOKENS // TOK_DEV)
    routes = jax.vmap(lambda own, number: deal_out(jax.random.fold_in(keys[1], 2), own, number, TOK_DEV, EXPERTS, 2, CAP, 2))(routes_keys, routes_turns).reshape((TOKENS, 2))
    route_weight = jnp.clip(jnp.exp(math.log(1.0) - 1.609438 * jax.random.uniform(keys[2], (TOKENS, 2), jnp.float32) ** level_of(keys[2], (TOKENS, 2), ((0, 32),), -0.2, 0.2)), 0.2, 1.0)
    gain = jnp.clip(1.0 + 0.18 * jax.random.normal(keys[3], (D,), jnp.float32), 0.1, 1.9)
    w_gate = gaussian(keys[4], (EXPERTS, D, FF), D ** -0.5, 0.125, ((1, 32), (2, 8)))
    w_up = gaussian(keys[5], (EXPERTS, D, FF), D ** -0.5, 0.125, ((1, 32), (2, 8)))
    w_down = gaussian(keys[6], (EXPERTS, D, FF), FF ** -0.5, 0.09375, ((1, 32), (2, 8)))
    return dict(tokens=tokens, routes=routes, route_weight=route_weight, gain=gain, w_gate=w_gate, w_up=w_up, w_down=w_down)


EPSILON = 1e-05

def expert_rows(pieces):
    rows, gate_w, up_w, down_w = pieces
    gate = jnp.dot(rows, gate_w, preferred_element_type=jnp.float32)
    upper = jnp.dot(rows, up_w, preferred_element_type=jnp.float32)
    hidden = (jax.nn.silu(gate) * upper).astype(jnp.bfloat16)
    count = rows.shape[0]
    blocked = hidden.reshape(count, N_TP, FF // N_TP).astype(jnp.float32)
    down_blocks = down_w.reshape(D, N_TP, FF // N_TP).astype(jnp.float32)
    partial_value = jnp.einsum('rjf,djf->jrd', blocked, down_blocks)
    rounded = lax.optimization_barrier(partial_value.astype(jnp.bfloat16))
    return lax.optimization_barrier(jnp.sum(rounded.astype(jnp.float32), axis=0)).astype(jnp.bfloat16)

def reference(tokens, routes, route_weight, gain, w_gate, w_up, w_down):
    scaling = gain[None, :, None]
    gate_out = (w_gate.astype(jnp.float32) * scaling).astype(jnp.bfloat16)
    up_out = (w_up.astype(jnp.float32) * scaling).astype(jnp.bfloat16)
    down_out = w_down
    float_rows = tokens.astype(jnp.float32)
    normed = (float_rows * lax.rsqrt(lax.optimization_barrier(jnp.mean(float_rows * float_rows, axis=-1, keepdims=True)) + EPSILON)).astype(jnp.bfloat16)
    groups = N_GR * N_FS
    flat_ids = routes.reshape(groups, TOK_DEV * 2)
    onehot = (flat_ids[:, :, None] == jnp.arange(EXPERTS, dtype=jnp.int32)[None, None, :]).astype(jnp.int32)
    slot_rank = lax.optimization_barrier(jnp.sum((jnp.cumsum(onehot, axis=1) - onehot) * onehot, axis=-1))
    group_ids = jnp.arange(groups, dtype=jnp.int32)[:, None]
    destination = (flat_ids * (groups * CAP) + group_ids * CAP + slot_rank).reshape(-1).astype(jnp.int32)
    token_ids = (jnp.arange(TOKENS * 2, dtype=jnp.int32) // 2).astype(jnp.int32)
    source = jnp.zeros((EXPERTS * groups * CAP,), jnp.int32).at[destination].set(token_ids)
    gathered = normed[source].reshape(EXPERTS, groups * CAP, D)
    outputs = lax.map(expert_rows, (gathered, gate_out, up_out, down_out))
    flat_out = outputs.reshape(EXPERTS * groups * CAP, D)
    picked = flat_out[destination].reshape(TOKENS, 2, D).astype(jnp.float32)
    mixed = lax.optimization_barrier(jnp.sum(route_weight[:, :, None] * picked, axis=1)).astype(jnp.bfloat16)
    return (gate_out, up_out, down_out, mixed)
```

```python
import jax
import jax.numpy as jnp
from jax import lax
from jax.sharding import PartitionSpec as P

D = 2048
EXP_DEV = 1


EPSILON = 1e-05


def sent_together(arrays, axis, split_dim, concat_dim, along):
    widths = [a.shape[along] for a in arrays]
    both = jnp.concatenate(arrays, axis=along)
    whole = lax.all_to_all(both, axis, split_axis=split_dim, concat_axis=concat_dim, tiled=True)
    return tuple(jnp.split(whole, [sum(widths[:k]) for k in range(1, len(widths))], axis=along))


def body(tokens, routes, route_weight, gain, w_gate, w_up, w_down):
    scaling = gain[None, :, None]
    gate_local = (w_gate * scaling).astype(jnp.bfloat16)
    up_local = (w_up * scaling).astype(jnp.bfloat16)
    gate_twice = jnp.concatenate([gate_local, gate_local], axis=0)
    up_twice = jnp.concatenate([up_local, up_local], axis=0)
    down_twice = jnp.concatenate([w_down, w_down], axis=0)
    fs_count = lax.axis_size("fs")
    experts = EXP_DEV * fs_count
    tok_rows = tokens.shape[0]
    capacity = 3 * tok_rows // experts
    float_rows = tokens.astype(jnp.float32)
    normed = (
        float_rows * lax.rsqrt(jnp.mean(float_rows * float_rows, axis=-1, keepdims=True) + EPSILON)
    ).astype(jnp.bfloat16)
    flat_ids = routes.reshape(-1)
    onehot = (flat_ids[:, None] == jnp.arange(experts, dtype=jnp.int32)[None, :]).astype(jnp.int32)
    slot_rank = jnp.sum((jnp.cumsum(onehot, axis=0) - onehot) * onehot, axis=-1)
    destination = (flat_ids * capacity + slot_rank).reshape(tok_rows, 2)
    slot_ids = jnp.arange(experts * capacity, dtype=jnp.int32)
    hits = slot_ids[:, None, None] == destination[None, :, :]
    dispatch = jnp.any(hits, axis=-1).astype(jnp.bfloat16)
    part = D // lax.axis_size("tp")
    mine = lax.dynamic_slice_in_dim(normed, lax.axis_index("tp") * part, part, axis=1)
    outgoing = jnp.dot(dispatch, mine, preferred_element_type=jnp.float32).astype(jnp.bfloat16)
    outgoing = outgoing.reshape(fs_count, EXP_DEV, capacity, part)
    arrived = lax.all_to_all(outgoing, "fs", split_axis=0, concat_axis=0, tiled=True)
    gate_twice, up_twice, down_twice, arrived = lax.optimization_barrier(
        (gate_twice, up_twice, down_twice, arrived)
    )
    arrived = lax.all_gather(arrived, "tp", axis=3, tiled=True)
    gate_out, up_out = sent_together((gate_twice, up_twice), ("gr", "fs"), 0, 1, 2)
    (down_out,) = sent_together((down_twice,), ("gr", "fs"), 0, 1, 2)

    def expert_work(arrived):
        gate = jnp.einsum("sjnd,jdf->sjnf", arrived, gate_out, preferred_element_type=jnp.float32)
        upper = jnp.einsum("sjnd,jdf->sjnf", arrived, up_out, preferred_element_type=jnp.float32)
        hidden = (jax.nn.silu(gate) * upper).astype(jnp.bfloat16)
        partial_value = jnp.einsum(
            "sjnf,jdf->sjnd", hidden, down_out, preferred_element_type=jnp.float32
        )
        rounded = lax.optimization_barrier(partial_value.astype(jnp.bfloat16))
        summed = lax.psum_scatter(
            rounded.astype(jnp.float32).astype(jnp.bfloat16), "tp", scatter_dimension=3, tiled=True
        )
        return summed

    results = expert_work(arrived)
    back_home = lax.all_to_all(results, "fs", split_axis=0, concat_axis=0, tiled=True)
    features = back_home.shape[-1]
    flat_back = back_home.reshape(experts * capacity, features).astype(jnp.float32)
    first = jnp.where(slot_ids[None, :] == destination[:, 0:1], route_weight[:, 0:1], 0.0)
    second = jnp.where(slot_ids[None, :] == destination[:, 1:2], route_weight[:, 1:2], 0.0)
    combine_map = first + second
    mixed = jnp.dot(combine_map, flat_back, preferred_element_type=jnp.float32).astype(jnp.bfloat16)
    return (gate_out, up_out, down_out, mixed)


def solution(mesh):
    in_specs = (
        P(("gr", "fs"), None),
        P(("gr", "fs"), None),
        P(("gr", "fs"), None),
        P(("gr", "fs")),
        P(None, ("gr", "fs"), "tp"),
        P(None, ("gr", "fs"), "tp"),
        P(None, ("gr", "fs"), "tp"),
    )
    out_specs = (
        P("fs", None, "tp"),
        P("fs", None, "tp"),
        P("fs", None, "tp"),
        P(("gr", "fs"), "tp"),
    )
    return jax.shard_map(body, mesh=mesh, in_specs=in_specs, out_specs=out_specs, check_vma=False)
```

```python
import functools

import jax
import jax.numpy as jnp
from jax import lax
from jax.experimental import pallas as pl
from jax.experimental.pallas import tpu as pltpu
from jax.sharding import PartitionSpec as P

MESH = pl.DeviceIdType.MESH
F32, BF16 = jnp.float32, jnp.bfloat16
EPSILON = 1e-05
D, UNITS, EXPERTS, TOK, CAP, TP, SOURCES = 2048, 512, 16, 512, 96, 8, 32
PART = D // TP
ROWS = EXPERTS * CAP
ROUNDS, HALF = 2, 128


def iota(shape, axis):
    return lax.broadcasted_iota(jnp.int32, shape, axis)


def kernel(
    tok_hbm, routes_ref, weight_ref, gain_ref, wg_hbm, wu_hbm, wd_hbm,
    go_hbm, uo_hbm, do_hbm, mixed_ref,
    tok, mine, normed, dest, cmap, gu, outgoing, gur, dn, rows, hidden,
    pair_out, pair_in, own, chip, ring_in, result, back,
    load_sem, self_sem, store_sem, gu_send, gu_recv, dn_send, dn_recv, tok_send, tok_recv,
    y_send, y_recv, core_send, core_recv, pair_send, pair_recv, ring_send, ring_recv, back_send, back_recv,
):
    gr, fs, tp = lax.axis_index("gr"), lax.axis_index("fs"), lax.axis_index("tp")
    z, x = gr * 4 + fs // 4, fs % 4
    y, core = tp // 2, tp % 2
    me = gr * 16 + fs
    odd = z % 2

    def plane(z2, x2):
        return {"gr": z2 // 4, "fs": (z2 % 4) * 4 + x2, "tp": tp}

    def peer(k):
        i, turn = k // 4, k % 4
        far = (i + 1) // 2
        step = (i % 2) * far + (1 - i % 2) * ((8 - far) % 8)
        return (z + step) % 8, (x + turn) % 4

    def column(y2, core2):
        return {"gr": gr, "fs": fs, "tp": y2 * 2 + core2}

    def remote(src, dst, send, recv, device):
        return pltpu.make_async_remote_copy(
            src_ref=src, dst_ref=dst, send_sem=send, recv_sem=recv, device_id=device, device_id_type=MESH
        )

    def drained(ref, sem):
        pltpu.make_async_copy(ref, ref, sem).wait()

    barrier = pltpu.get_barrier_semaphore()

    def greet(k, carry):
        pl.semaphore_signal(barrier, inc=1, device_id=plane(*peer(k)), device_id_type=MESH)
        return carry

    lax.fori_loop(1, 32, greet, 0)
    for turn in range(1, 4):
        pl.semaphore_signal(barrier, inc=1, device_id=column((y + turn) % 4, core), device_id_type=MESH)
    pl.semaphore_signal(barrier, inc=1, device_id=column(y, 1 - core), device_id_type=MESH)

    loads = [
        pltpu.make_async_copy(wg_hbm, gu.at[:, 0], load_sem.at[0]),
        pltpu.make_async_copy(wu_hbm, gu.at[:, 1], load_sem.at[1]),
        pltpu.make_async_copy(tok_hbm, tok, load_sem.at[2]),
        pltpu.make_async_copy(tok_hbm.at[:, pl.ds(pl.multiple_of(tp * PART, PART), PART)], mine, load_sem.at[3]),
    ]
    for load in loads:
        load.start()

    r0, r1 = routes_ref[0:1, :].astype(F32), routes_ref[1:2, :].astype(F32)
    names = iota((EXPERTS, TOK), 0).astype(F32)
    named = jnp.where((names == r0) | (names == r1), 1.0, 0.0)
    earlier = jnp.where(iota((TOK, TOK), 0) < iota((TOK, TOK), 1), 1.0, 0.0).astype(BF16)
    rank = jnp.dot(named.astype(BF16), earlier, preferred_element_type=F32)
    dest[0:1, :] = r0 * CAP + jnp.sum(jnp.where(names == r0, rank, 0.0), axis=0, keepdims=True)
    dest[1:2, :] = r1 * CAP + jnp.sum(jnp.where(names == r1, rank, 0.0), axis=0, keepdims=True)

    diagonal = iota((64, 64), 0) == iota((64, 64), 1)
    gain = jnp.sum(jnp.where(diagonal, gain_ref[...], 0.0), axis=1, keepdims=True)
    loads[0].wait()
    loads[1].wait()

    def scale(e, carry):
        for m in range(2):
            gu[e, m] = (gu[e, m].astype(F32) * gain).astype(BF16)
        return carry

    lax.fori_loop(0, EXPERTS, scale, 0)

    loads[2].wait()
    loads[3].wait()

    def norm(b, carry):
        at = pl.ds(pl.multiple_of(b * 64, 64), 64)
        full = tok[at, :].astype(F32)
        inverse = lax.rsqrt(jnp.mean(full * full, axis=-1, keepdims=True) + EPSILON)
        normed[at, :] = (mine[at, :].astype(F32) * inverse).astype(BF16)
        return carry

    lax.fori_loop(0, TOK // 64, norm, 0)

    def pick(e, carry):
        slot = (iota((CAP, TOK), 0) + e * CAP).astype(F32)
        hits = jnp.where((slot == dest[0:1, :]) | (slot == dest[1:2, :]), 1.0, 0.0).astype(BF16)
        outgoing[e] = jnp.dot(hits, normed[...], preferred_element_type=F32).astype(BF16)
        return carry

    lax.fori_loop(0, EXPERTS, pick, 0)

    pl.semaphore_wait(barrier, 35)

    def slot_at(z2, z1):
        return (z1 - z2 + 2 - z2 % 2 + 16) % 8

    home = slot_at(z, z) * 4 + x

    def block(slot):
        return pl.ds(pl.multiple_of(slot * CAP, CAP), CAP)

    steps = [0, 1, 7, (1 - odd) * 2 + odd * 6]
    tok_self = pltpu.make_async_copy(outgoing.at[fs], rows.at[tp, block(home)], self_sem.at[0])
    tok_self.start()
    for i in range(4):
        for turn in range(4):
            if i + turn:
                z2, x2 = (z + steps[i]) % 8, (x + turn) % 4
                remote(
                    outgoing.at[(z2 % 4) * 4 + x2], rows.at[tp, block(slot_at(z2, z) * 4 + x)],
                    tok_send, tok_recv, plane(z2, x2),
                ).start()

    gu_self = pltpu.make_async_copy(gu.at[fs], gur.at[me], self_sem.at[1])
    gu_self.start()
    dn_self = [
        pltpu.make_async_copy(wd_hbm.at[fs, pl.ds(r * 32, 32)], dn.at[r, me], self_sem.at[2 + r]) for r in range(ROUNDS)
    ]
    for copy in dn_self:
        copy.start()

    def send_gu(k, carry):
        z2, x2 = peer(k)
        remote(gu.at[(z2 % 4) * 4 + x2], gur.at[me], gu_send, gu_recv, plane(z2, x2)).start()
        return carry

    lax.fori_loop(1, 32, send_gu, 0)

    for r in range(ROUNDS):
        def send_dn(k, carry):
            z2, x2 = peer(k)
            remote(
                wd_hbm.at[(z2 % 4) * 4 + x2, pl.ds(r * 32, 32)], dn.at[r, me],
                dn_send.at[r], dn_recv.at[r], plane(z2, x2),
            ).start()
            return carry

        lax.fori_loop(1, 32, send_dn, 0)

    across = iota((TOK, TOK), 0) == iota((TOK, TOK), 1)

    def upright(row):
        return jnp.sum(jnp.where(across, row, 0.0), axis=1, keepdims=True)

    mine_cols = jnp.concatenate(
        [upright(dest[0:1, :]), upright(dest[1:2, :]), upright(weight_ref[0:1, :]), upright(weight_ref[1:2, :])], axis=1
    )
    for b in range(8):
        cols = mine_cols[b * 64 : (b + 1) * 64]
        slot = iota((64, ROWS), 1).astype(F32)
        cmap[b * 64 : (b + 1) * 64, :] = (
            jnp.where(slot == cols[:, 0:1], cols[:, 2:3], 0.0) + jnp.where(slot == cols[:, 1:2], cols[:, 3:4], 0.0)
        ).astype(BF16)

    tok_self.wait()
    drained(outgoing.at[0:15], tok_recv)
    turns = (1, 3, 2)
    y_copies = [
        remote(rows.at[tp], rows.at[tp], y_send.at[turn - 1], y_recv.at[turn - 1], column((y + turn) % 4, core))
        for turn in turns
    ]
    for copy in y_copies:
        copy.start()
    core_copies = [remote(rows.at[tp], rows.at[tp], core_send.at[0], core_recv.at[0], column(y, 1 - core))]
    core_copies[0].start()
    for turn in turns:
        origin = ((y - turn + 4) % 4) * 2 + core
        drained(rows.at[origin], y_recv.at[turn - 1])
        core_copies.append(
            remote(rows.at[origin], rows.at[origin], core_send.at[turn], core_recv.at[turn], column(y, 1 - core))
        )
        core_copies[-1].start()
    for copy in core_copies:
        copy.wait_recv()

    gu_self.wait()
    drained(gur.at[0:31], gu_recv)
    stores = [
        pltpu.make_async_copy(gur.at[:, 0], go_hbm, store_sem.at[0]),
        pltpu.make_async_copy(gur.at[:, 1], uo_hbm, store_sem.at[1]),
    ]
    for store in stores:
        store.start()

    def units(m, carry):
        at = pl.ds(pl.multiple_of(m * 512, 512), 512)
        gate, upper = jnp.zeros((512, UNITS), F32), jnp.zeros((512, UNITS), F32)
        for j in range(TP):
            lhs = rows[j, at, :]
            gate += jnp.dot(lhs, gur[4 * j : 4 * j + 4, 0].reshape(PART, UNITS), preferred_element_type=F32)
            upper += jnp.dot(lhs, gur[4 * j : 4 * j + 4, 1].reshape(PART, UNITS), preferred_element_type=F32)
        hidden[at, :] = (gate / (1.0 + jnp.exp(-gate)) * upper).astype(BF16)
        return carry

    lax.fori_loop(0, ROWS // 512, units, 0)

    pair_copies, ring_copies = [], []
    for r in range(ROUNDS):
        dn_self[r].wait()
        drained(dn.at[r, 0:31], dn_recv.at[r])
        stores.append(pltpu.make_async_copy(dn.at[r], do_hbm.at[:, pl.ds(r * 32, 32)], store_sem.at[2 + r]))
        stores[-1].start()

        def partial(parity, two, store):
            def some(m, carry):
                at = pl.ds(pl.multiple_of(m * 512, 512), 512)
                down = jnp.concatenate(
                    [
                        dn[r, pl.ds(4 * (2 * (2 * two + k) + parity), 4)].reshape(HALF, UNITS)
                        for k in range(2)
                    ],
                    axis=0,
                )
                out = lax.dot_general(
                    hidden[at, :], down, (((1,), (1,)), ((), ())), preferred_element_type=F32
                )
                for k in range(2):
                    store(2 * two + k, at, out[:, k * HALF : (k + 1) * HALF])
                return carry

            lax.fori_loop(0, ROWS // 512, some, 0)

        def give(y2, at, value):
            pair_out[r, y2, at, :] = value.astype(BF16)

        def keep(y2, at, value):
            own[r, y2, at, :] = value

        for two in range(2):
            partial(1 - core, two, give)
            for y2 in (2 * two, 2 * two + 1):
                pair_copies.append(
                    remote(
                        pair_out.at[r, y2], pair_in.at[r, y2], pair_send.at[r, y2], pair_recv.at[r, y2],
                        column(y, 1 - core),
                    )
                )
                pair_copies[-1].start()
        for two in range(2):
            partial(core, two, keep)
        for y2 in range(4):
            pair_copies[4 * r + y2].wait_recv()
        for turn in (1, 3, 2, 0):
            y2 = (y + turn) % 4

            def both(m, carry):
                at = pl.ds(pl.multiple_of(m * 256, 256), 256)
                chip[r, y2, at, :] = (own[r, y2, at, :] + pair_in[r, y2, at, :].astype(F32)).astype(BF16)
                return carry

            lax.fori_loop(0, ROWS // 256, both, 0)
            if turn:
                ring_copies.append(
                    remote(
                        chip.at[r, y2], ring_in.at[r, turn - 1], ring_send.at[r, turn - 1], ring_recv.at[r, turn - 1],
                        column(y2, core),
                    )
                )
                ring_copies[-1].start()
        for copy in ring_copies[3 * r :]:
            copy.wait_recv()

        def total(m, carry):
            at = pl.ds(pl.multiple_of(m * 256, 256), 256)
            value = chip[r, y, at, :].astype(F32)
            for turn in range(3):
                value += ring_in[r, turn, at, :].astype(F32)
            result[r, at, :] = value.astype(BF16)
            return carry

        lax.fori_loop(0, ROWS // 256, total, 0)

        stores.append(pltpu.make_async_copy(result.at[r, block(home)], back.at[r, fs], self_sem.at[4 + r]))
        stores[-1].start()
        backs = [0, 1, 7, (1 - odd) * 6 + odd * 2]
        for i in (3, 1, 2, 0):
            for turn in range(4):
                if i + turn:
                    z1, x1 = (z + backs[i]) % 8, (x + turn) % 4
                    remote(
                        result.at[r, block(slot_at(z, z1) * 4 + x1)], back.at[r, fs],
                        back_send.at[r], back_recv.at[r], plane(z1, x1),
                    ).start()

    for store in stores:
        store.wait()
    mixes = []
    for r in range(ROUNDS):
        drained(back.at[r, 0:15], back_recv.at[r])
        mixes.append(jnp.dot(cmap[...], back[r].reshape(ROWS, HALF), preferred_element_type=F32).astype(BF16))
    mixed = jnp.concatenate(mixes, axis=1)
    a, b = iota((PART, PART), 0), iota((PART, PART), 1)
    order = jnp.where((a % HALF) // 32 * 64 + a // HALF * 32 + a % 32 == b, 1.0, 0.0).astype(BF16)
    mixed_ref[...] = jnp.dot(mixed, order, preferred_element_type=F32).astype(BF16)

    drained(outgoing.at[0:15], tok_send)
    drained(gur.at[0:31], gu_send)
    for r in range(ROUNDS):
        drained(dn.at[r, 0:31], dn_send.at[r])
        drained(back.at[r, 0:15], back_send.at[r])
    for copy in y_copies + core_copies + pair_copies + ring_copies:
        copy.wait_send()


def body(tokens, routes, route_weight, gain, w_gate, w_up, w_down):
    anywhere = pl.BlockSpec(memory_space=pl.ANY)
    vmem = pl.BlockSpec(memory_space=pltpu.VMEM)
    weights = jax.ShapeDtypeStruct((SOURCES, 64, UNITS), BF16)
    dma = pltpu.SemaphoreType.DMA
    gate_out, up_out, down_out, mixed = pl.pallas_call(
        kernel,
        out_shape=(weights, weights, weights, jax.ShapeDtypeStruct((TOK, PART), BF16)),
        in_specs=[anywhere, vmem, vmem, vmem, anywhere, anywhere, anywhere],
        out_specs=(anywhere, anywhere, anywhere, vmem),
        scratch_shapes=[
            pltpu.VMEM((TOK, D), BF16),
            pltpu.VMEM((TOK, PART), BF16),
            pltpu.VMEM((TOK, PART), BF16),
            pltpu.VMEM((2, TOK), F32),
            pltpu.VMEM((TOK, ROWS), BF16),
            pltpu.VMEM((EXPERTS, 2, 64, UNITS), BF16),
            pltpu.VMEM((EXPERTS, CAP, PART), BF16),
            pltpu.VMEM((SOURCES, 2, 64, UNITS), BF16),
            pltpu.VMEM((ROUNDS, SOURCES, 32, UNITS), BF16),
            pltpu.VMEM((TP, ROWS, PART), BF16),
            pltpu.VMEM((ROWS, UNITS), BF16),
            pltpu.VMEM((ROUNDS, 4, ROWS, HALF), BF16),
            pltpu.VMEM((ROUNDS, 4, ROWS, HALF), BF16),
            pltpu.VMEM((ROUNDS, 4, ROWS, HALF), F32),
            pltpu.VMEM((ROUNDS, 4, ROWS, HALF), BF16),
            pltpu.VMEM((ROUNDS, 3, ROWS, HALF), BF16),
            pltpu.VMEM((ROUNDS, ROWS, HALF), BF16),
            pltpu.VMEM((ROUNDS, EXPERTS, CAP, HALF), BF16),
            dma((4,)),
            dma((6,)),
            dma((4,)),
            dma, dma,
            dma((ROUNDS,)), dma((ROUNDS,)),
            dma, dma,
            dma((3,)), dma((3,)),
            dma((4,)), dma((4,)),
            dma((ROUNDS, 4)), dma((ROUNDS, 4)),
            dma((ROUNDS, 3)), dma((ROUNDS, 3)),
            dma((ROUNDS,)), dma((ROUNDS,)),
        ],
        compiler_params=pltpu.CompilerParams(
            collective_id=0, has_side_effects=True, vmem_limit_bytes=60 * 1024 * 1024
        ),
    )(tokens, routes.T, route_weight.T, gain.reshape(1, -1), w_gate, w_up, w_down)
    return tuple(w.reshape(1, D, UNITS) for w in (gate_out, up_out, down_out)) + (mixed,)


def solution(mesh):
    rows = ("gr", "fs")
    weights = P(None, rows, "tp")
    placed = P("fs", None, "tp")
    return jax.shard_map(
        body,
        mesh=mesh,
        in_specs=(P(rows, None), P(rows, None), P(rows, None), P(rows), weights, weights, weights),
        out_specs=(placed, placed, placed, P(rows, "tp")),
        check_vma=False,
    )
```

```python
import functools

import jax
import jax.numpy as jnp
from jax import lax
from jax.experimental import pallas as pl
from jax.experimental.pallas import tpu as pltpu
from jax.sharding import PartitionSpec as P

MESH = pl.DeviceIdType.MESH
F32, BF16 = jnp.float32, jnp.bfloat16
EPSILON = 1e-05
D, UNITS, EXPERTS, TOK, CAP, TP, SOURCES = 2048, 512, 16, 512, 96, 8, 32
PART = D // TP
ROWS = EXPERTS * CAP
ROUNDS, DEPTH, LANES = 4, 16, 128
PACKED = ROWS // 2
EARLY = 12


def iota(shape, axis):
    return lax.broadcasted_iota(jnp.int32, shape, axis)


def kernel(
    tok_hbm, routes_hbm, weight_hbm, gain_hbm, wg_hbm, wu_hbm, wd_hbm,
    gate_in, up_in, down_in, mixed_ref,
    routes_ref, weight_ref, gain_ref, tok, mine, normed, dest, cmap, gate_own, up_own, outgoing, rows, hidden,
    pair_out, pair_in, own, chip, relay, merged, ring_in, result, back,
    load_sem, self_sem, gu_send, gu_recv, dn_send, dn_recv, tok_send, tok_recv,
    y_send, y_recv, core_send, core_recv, pair_send, pair_recv, ring_send, ring_recv, back_send, back_recv,
):
    gr, fs, tp = lax.axis_index("gr"), lax.axis_index("fs"), lax.axis_index("tp")
    z, x = gr * 4 + fs // 4, fs % 4
    y, core = tp // 2, tp % 2
    me = gr * 16 + fs
    odd = z % 2

    def plane(z2, x2):
        return {"gr": z2 // 4, "fs": (z2 % 4) * 4 + x2, "tp": tp}

    def peer(k):
        i, turn = k // 4, k % 4
        far = (i + 1) // 2
        step = (i % 2) * far + (1 - i % 2) * ((8 - far) % 8)
        turn = (i % 2) * turn + (1 - i % 2) * ((4 - turn) % 4)
        return (z + step) % 8, (x + turn) % 4

    def column(y2, core2):
        return {"gr": gr, "fs": fs, "tp": y2 * 2 + core2}

    def remote(src, dst, send, recv, device):
        return pltpu.make_async_remote_copy(
            src_ref=src, dst_ref=dst, send_sem=send, recv_sem=recv, device_id=device, device_id_type=MESH
        )

    def drained(ref, sem):
        pltpu.make_async_copy(ref, ref, sem).wait()

    barrier = pltpu.get_barrier_semaphore()

    def greet(k, carry):
        pl.semaphore_signal(barrier, inc=1, device_id=plane(*peer(32 - k)), device_id_type=MESH)
        return carry

    lax.fori_loop(1, 32, greet, 0)
    for turn in range(1, 4):
        pl.semaphore_signal(barrier, inc=1, device_id=column((y + turn) % 4, core), device_id_type=MESH)
    pl.semaphore_signal(barrier, inc=1, device_id=column(y, 1 - core), device_id_type=MESH)

    loads = [
        pltpu.make_async_copy(wg_hbm, gate_own, load_sem.at[0]),
        pltpu.make_async_copy(wu_hbm, up_own, load_sem.at[1]),
        pltpu.make_async_copy(tok_hbm, tok, load_sem.at[2]),
        pltpu.make_async_copy(tok_hbm.at[:, pl.ds(pl.multiple_of(tp * PART, PART), PART)], mine, load_sem.at[3]),
    ]
    loads += [
        pltpu.make_async_copy(src, dst, load_sem.at[4 + n])
        for n, (src, dst) in enumerate(((routes_hbm, routes_ref), (weight_hbm, weight_ref), (gain_hbm, gain_ref)))
    ]
    for load in loads:
        load.start()

    for load in loads[4:]:
        load.wait()
    diagonal = iota((64, 64), 0) == iota((64, 64), 1)
    gain = jnp.sum(jnp.where(diagonal, gain_ref[...], 0.0), axis=1, keepdims=True)
    loads[0].wait()
    loads[1].wait()

    def scale(e, carry):
        for ref in (gate_own, up_own):
            ref[e] = (ref[e].astype(F32) * gain).astype(BF16)
        return carry

    lax.fori_loop(0, EXPERTS, scale, 0)

    r0, r1 = routes_ref[0:1, :].astype(F32), routes_ref[1:2, :].astype(F32)
    names = iota((EXPERTS, TOK), 0).astype(F32)
    named = jnp.where((names == r0) | (names == r1), 1.0, 0.0)
    earlier = jnp.where(iota((TOK, TOK), 0) < iota((TOK, TOK), 1), 1.0, 0.0).astype(BF16)
    ranks = jnp.dot(named.astype(BF16), earlier, preferred_element_type=F32)
    for k, name in enumerate((r0, r1)):
        rank = jnp.sum(jnp.where(names == name, ranks, 0.0), axis=0, keepdims=True)
        dest[k : k + 1, :] = name * CAP + rank
        late = jnp.where(rank >= CAP // 2, float(PACKED - CAP // 2), 0.0)
        dest[2 + k : 3 + k, :] = name * (CAP // 2) + rank + late

    pl.semaphore_wait(barrier, 35)

    def send_gu(k, carry):
        z2, x2 = peer(k)
        e = (z2 % 4) * 4 + x2
        remote(gate_own.at[e], gate_in.at[me], gu_send.at[0], gu_recv.at[0], plane(z2, x2)).start()
        remote(up_own.at[e], up_in.at[me], gu_send.at[1], gu_recv.at[1], plane(z2, x2)).start()
        return carry

    lax.fori_loop(1, EARLY, send_gu, 0)

    loads[2].wait()
    loads[3].wait()

    def norm(b, carry):
        at = pl.ds(pl.multiple_of(b * 64, 64), 64)
        full = tok[at, :].astype(F32)
        inverse = lax.rsqrt(jnp.mean(full * full, axis=-1, keepdims=True) + EPSILON)
        normed[at, :] = (mine[at, :].astype(F32) * inverse).astype(BF16)
        return carry

    lax.fori_loop(0, TOK // 64, norm, 0)

    def pick(e, carry):
        slot = (iota((CAP, TOK), 0) + e * CAP).astype(F32)
        hits = jnp.where((slot == dest[0:1, :]) | (slot == dest[1:2, :]), 1.0, 0.0).astype(BF16)
        outgoing[e] = jnp.dot(hits, normed[...], preferred_element_type=F32).astype(BF16)
        return carry

    lax.fori_loop(0, EXPERTS, pick, 0)

    def slot_at(z2, z1):
        return (z1 - z2 + 2 - z2 % 2 + 16) % 8

    home = slot_at(z, z) * 4 + x

    def block(slot):
        return pl.ds(pl.multiple_of(slot * CAP, CAP), CAP)

    steps = [0, 1, 7, (1 - odd) * 2 + odd * 6]
    tok_self = pltpu.make_async_copy(outgoing.at[fs], rows.at[tp, block(home)], self_sem.at[0])
    tok_self.start()
    for i in range(4):
        for turn in range(4):
            if i + turn:
                z2, x2 = (z + steps[i]) % 8, (x + turn) % 4
                remote(
                    outgoing.at[(z2 % 4) * 4 + x2], rows.at[tp, block(slot_at(z2, z) * 4 + x)],
                    tok_send, tok_recv, plane(z2, x2),
                ).start()

    selves = [
        pltpu.make_async_copy(gate_own.at[fs], gate_in.at[me], self_sem.at[1]),
        pltpu.make_async_copy(up_own.at[fs], up_in.at[me], self_sem.at[2]),
        pltpu.make_async_copy(wd_hbm.at[fs], down_in.at[me], self_sem.at[3]),
    ]
    for copy in selves:
        copy.start()

    lax.fori_loop(EARLY, 32, send_gu, 0)

    def band(r):
        return pl.ds(pl.multiple_of(r * DEPTH, DEPTH), DEPTH)

    def send_dn(n, carry):
        r, k = n // 31, n % 31 + 1
        z2, x2 = peer(k)
        remote(
            wd_hbm.at[(z2 % 4) * 4 + x2, band(r)], down_in.at[me, band(r)],
            dn_send, dn_recv.at[r], plane(z2, x2),
        ).start()
        return carry

    lax.fori_loop(0, 31 * ROUNDS, send_dn, 0)

    across = iota((TOK, TOK), 0) == iota((TOK, TOK), 1)

    def upright(row):
        return jnp.sum(jnp.where(across, row, 0.0), axis=1, keepdims=True)

    mine_cols = jnp.concatenate(
        [upright(dest[2:3, :]), upright(dest[3:4, :]), upright(weight_ref[0:1, :]), upright(weight_ref[1:2, :])], axis=1
    )
    for b in range(8):
        cols = mine_cols[b * 64 : (b + 1) * 64]
        slot = iota((64, ROWS), 1).astype(F32)
        cmap[b * 64 : (b + 1) * 64, :] = (
            jnp.where(slot == cols[:, 0:1], cols[:, 2:3], 0.0) + jnp.where(slot == cols[:, 1:2], cols[:, 3:4], 0.0)
        ).astype(BF16)

    tok_self.wait()
    drained(outgoing.at[0:15], tok_recv)
    turns = (1, 3, 2)
    y_copies = [
        remote(rows.at[tp], rows.at[tp], y_send.at[turn - 1], y_recv.at[turn - 1], column((y + turn) % 4, core))
        for turn in turns
    ]
    for copy in y_copies:
        copy.start()
    core_copies = [remote(rows.at[tp], rows.at[tp], core_send.at[0], core_recv.at[0], column(y, 1 - core))]
    core_copies[0].start()
    for turn in turns:
        origin = ((y - turn + 4) % 4) * 2 + core
        drained(rows.at[origin], y_recv.at[turn - 1])
        core_copies.append(
            remote(rows.at[origin], rows.at[origin], core_send.at[turn], core_recv.at[turn], column(y, 1 - core))
        )
        core_copies[-1].start()
    for copy in core_copies:
        copy.wait_recv()

    for copy in selves:
        copy.wait()
    drained(gate_in.at[0:31], gu_recv.at[0])
    drained(up_in.at[0:31], gu_recv.at[1])

    def units(m, carry):
        at = pl.ds(pl.multiple_of(m * 4 * CAP, 4 * CAP), 4 * CAP)
        gate, upper = jnp.zeros((4 * CAP, UNITS), F32), jnp.zeros((4 * CAP, UNITS), F32)
        for j in range(TP):
            lhs = rows[j, at, :]
            gate += jnp.dot(lhs, gate_in[4 * j : 4 * j + 4].reshape(PART, UNITS), preferred_element_type=F32)
            upper += jnp.dot(lhs, up_in[4 * j : 4 * j + 4].reshape(PART, UNITS), preferred_element_type=F32)
        value = (gate / (1.0 + jnp.exp(-gate)) * upper).astype(BF16).reshape(4, 2, CAP // 2, UNITS)
        for half in range(2):
            hidden[half, pl.ds(4 * m, 4)] = value[:, half]
        return carry

    lax.fori_loop(0, EXPERTS // 4, units, 0)

    left = iota((8 * CAP // 2, LANES), 1) < LANES // 2
    pair_copies, ring_copies = [], []

    def half_block(slot):
        return pl.ds(pl.multiple_of(slot * (CAP // 2), CAP // 2), CAP // 2)

    def sum_cores(r):
        drained(down_in.at[0:31, 0:DEPTH], dn_recv.at[r])

        def partial(parity, store):
            down = jnp.concatenate(
                [
                    down_in[pl.ds(4 * (2 * k + parity), 4), r * DEPTH : (r + 1) * DEPTH].reshape(4 * DEPTH, UNITS)
                    for k in range(4)
                ],
                axis=0,
            )

            for m in range(2):
                outs = [
                    lax.dot_general(
                        hidden[half, 8 * m : 8 * m + 8].reshape(4 * CAP, UNITS), down, (((1,), (1,)), ((), ())),
                        preferred_element_type=F32,
                    )
                    for half in range(2)
                ]
                for two in range(2):
                    lanes = slice(two * LANES, (two + 1) * LANES)
                    low, high = outs[0][:, lanes], outs[1][:, lanes]
                    at = slice(m * 4 * CAP, (m + 1) * 4 * CAP)
                    store(2 * two, at, jnp.where(left, low, pltpu.roll(high, LANES // 2, 1)))
                    store(2 * two + 1, at, jnp.where(left, pltpu.roll(low, LANES // 2, 1), high))

        def give(y2, at, value):
            pair_out[r, y2, at, :] = value.astype(BF16)

        def keep(y2, at, value):
            own[r, y2, at, :] = value

        partial(1 - core, give)
        for turn in (2, 1, 3, 0):
            y2 = (y + turn) % 4
            pair_copies.append(
                remote(
                    pair_out.at[r, y2], pair_in.at[r, y2], pair_send.at[r, y2], pair_recv.at[r, y2],
                    column(y, 1 - core),
                )
            )
            pair_copies[-1].start()
        partial(core, keep)
        low, high = slice(0, PACKED // 2), slice(PACKED // 2, PACKED)
        sides = ((0, (y + 1) % 4, low, high), (1, (y + 3) % 4, high, low))

        def ring(n, src, dst, device):
            ring_copies.append(remote(src, dst, ring_send.at[r, n], ring_recv.at[r, n], device))
            ring_copies[-1].start()

        for n, turn in enumerate((2, 1, 3, 0)):
            y2 = (y + turn) % 4
            pair_copies[4 * r + n].wait_recv()
            chip[r, y2] = (own[r, y2] + pair_in[r, y2].astype(F32)).astype(BF16)
            if turn == 2:
                for n, near, first, _ in sides:
                    ring(n, chip.at[r, y2, first], relay.at[r, n], column(near, core))
        for n, near, _, second in sides:
            ring(2 + n, chip.at[r, near, second], ring_in.at[r, n, second], column(near, core))
        for n, near, first, _ in sides:
            ring_copies[6 * r + n].wait_recv()
            merged[r, n] = (chip[r, near, first].astype(F32) + relay[r, n].astype(F32)).astype(BF16)
            ring(4 + n, merged.at[r, n], ring_in.at[r, n, first], column(near, core))

    def sum_chips(r):
        for copy in ring_copies[6 * r + 2 : 6 * r + 6]:
            copy.wait_recv()
        value = chip[r, y].astype(F32)
        for n in range(2):
            value += ring_in[r, n].astype(F32)
        result[r] = value.astype(BF16)
        selves.append(pltpu.make_async_copy(result.at[r, half_block(home)], back.at[r, fs], self_sem.at[4 + r]))
        selves[-1].start()
        backs = [0, 1, 7, (1 - odd) * 6 + odd * 2]
        for i in (3, 1, 2, 0):
            for turn in range(4):
                if i + turn:
                    z1, x1 = (z + backs[i]) % 8, (x + turn) % 4
                    remote(
                        result.at[r, half_block(slot_at(z, z1) * 4 + x1)], back.at[r, fs],
                        back_send.at[r], back_recv.at[r], plane(z1, x1),
                    ).start()

    for r in range(ROUNDS):
        sum_cores(r)
        if r:
            sum_chips(r - 1)
    sum_chips(ROUNDS - 1)

    mixes = []
    for r in range(ROUNDS):
        selves[3 + r].wait()
        drained(back.at[r, 0:15], back_recv.at[r])
        returned = back[r].reshape(PACKED, LANES)
        low = jnp.dot(cmap[:, :PACKED], returned, preferred_element_type=F32)
        high = jnp.dot(cmap[:, PACKED:], returned, preferred_element_type=F32)
        mixes.append(low + pltpu.roll(high, LANES // 2, 1))
    first = iota((TOK, LANES), 1) < LANES // 2
    mixed = jnp.concatenate(
        [jnp.where(first, mixes[k], pltpu.roll(mixes[k + 1], LANES // 2, 1)) for k in (0, 2)], axis=1
    ).astype(BF16)
    a, b = iota((PART, PART), 0), iota((PART, PART), 1)
    order = jnp.where((a % 64) // DEPTH * 64 + a // 64 * DEPTH + a % DEPTH == b, 1.0, 0.0).astype(BF16)
    mixed_ref[...] = jnp.dot(mixed, order, preferred_element_type=F32).astype(BF16)

    drained(outgoing.at[0:15], tok_send)
    drained(gate_in.at[0:31], gu_send.at[0])
    drained(up_in.at[0:31], gu_send.at[1])
    drained(down_in.at[0:31], dn_send)
    for r in range(ROUNDS):
        drained(back.at[r, 0:15], back_send.at[r])
    for copy in y_copies + core_copies + pair_copies + ring_copies:
        copy.wait_send()


def body(tokens, routes, route_weight, gain, w_gate, w_up, w_down):
    anywhere = pl.BlockSpec(memory_space=pl.ANY)
    vmem = pl.BlockSpec(memory_space=pltpu.VMEM)
    weights = pltpu.VMEM((SOURCES, 64, UNITS), BF16)
    dma = pltpu.SemaphoreType.DMA
    gate_out, up_out, down_out, mixed = pl.pallas_call(
        kernel,
        out_shape=(weights, weights, weights, pltpu.VMEM((TOK, PART), BF16)),
        in_specs=[anywhere] * 7,
        out_specs=(vmem, vmem, vmem, vmem),
        scratch_shapes=[
            pltpu.VMEM((2, TOK), jnp.int32),
            pltpu.VMEM((2, TOK), F32),
            pltpu.VMEM((1, D // SOURCES), F32),
            pltpu.VMEM((TOK, D), BF16),
            pltpu.VMEM((TOK, PART), BF16),
            pltpu.VMEM((TOK, PART), BF16),
            pltpu.VMEM((4, TOK), F32),
            pltpu.VMEM((TOK, ROWS), BF16),
            pltpu.VMEM((EXPERTS, 64, UNITS), BF16),
            pltpu.VMEM((EXPERTS, 64, UNITS), BF16),
            pltpu.VMEM((EXPERTS, CAP, PART), BF16),
            pltpu.VMEM((TP, ROWS, PART), BF16),
            pltpu.VMEM((2, EXPERTS, CAP // 2, UNITS), BF16),
            pltpu.VMEM((ROUNDS, 4, PACKED, LANES), BF16),
            pltpu.VMEM((ROUNDS, 4, PACKED, LANES), BF16),
            pltpu.VMEM((ROUNDS, 4, PACKED, LANES), F32),
            pltpu.VMEM((ROUNDS, 4, PACKED, LANES), BF16),
            pltpu.VMEM((ROUNDS, 2, PACKED // 2, LANES), BF16),
            pltpu.VMEM((ROUNDS, 2, PACKED // 2, LANES), BF16),
            pltpu.VMEM((ROUNDS, 2, PACKED, LANES), BF16),
            pltpu.VMEM((ROUNDS, PACKED, LANES), BF16),
            pltpu.VMEM((ROUNDS, EXPERTS, CAP // 2, LANES), BF16),
            dma((7,)),
            dma((8,)),
            dma((2,)), dma((2,)),
            dma, dma((ROUNDS,)),
            dma, dma,
            dma((3,)), dma((3,)),
            dma((4,)), dma((4,)),
            dma((ROUNDS, 4)), dma((ROUNDS, 4)),
            dma((ROUNDS, 6)), dma((ROUNDS, 6)),
            dma((ROUNDS,)), dma((ROUNDS,)),
        ],
        compiler_params=pltpu.CompilerParams(
            collective_id=0, has_side_effects=True, vmem_limit_bytes=52 * 1024 * 1024
        ),
    )(tokens, routes.T, route_weight.T, gain.reshape(1, -1), w_gate, w_up, w_down)
    return tuple(w.reshape(1, D, UNITS) for w in (gate_out, up_out, down_out)) + (mixed,)


def solution(mesh):
    rows = ("gr", "fs")
    weights = P(None, rows, "tp")
    placed = P("fs", None, "tp")
    return jax.shard_map(
        body,
        mesh=mesh,
        in_specs=(P(rows, None), P(rows, None), P(rows, None), P(rows), weights, weights, weights),
        out_specs=(placed, placed, placed, P(rows, "tp")),
        check_vma=False,
    )
```

```python
import functools

import jax
import jax.numpy as jnp
from jax import lax
from jax.experimental import pallas as pl
from jax.experimental.pallas import tpu as pltpu
from jax.sharding import PartitionSpec as P

MESH = pl.DeviceIdType.MESH
F32, BF16 = jnp.float32, jnp.bfloat16
EPSILON = 1e-05
D, UNITS, EXPERTS, TOK, CAP, TP, SOURCES = 2048, 512, 16, 512, 96, 8, 32
PART = D // TP
ROWS = EXPERTS * CAP
ROUNDS, DEPTH, LANES = 4, 16, 128
PACKED = ROWS // 2
EARLY = 12


def iota(shape, axis):
    return lax.broadcasted_iota(jnp.int32, shape, axis)


def mix_of(cmap, returned):
    returned = returned.reshape(PACKED, LANES)
    low = jnp.dot(cmap[:, :PACKED], returned, preferred_element_type=F32)
    high = jnp.dot(cmap[:, PACKED:], returned, preferred_element_type=F32)
    return low + pltpu.roll(high, LANES // 2, 1)


def in_lanes(one, other):
    first = iota((TOK, LANES), 1) < LANES // 2
    return jnp.where(first, one, pltpu.roll(other, LANES // 2, 1))


def finish(gate_in, up_in, down_in, cmap, begun_ref, back_ref, gate_hbm, up_hbm, down_hbm, mixed_hbm, mixed, sem):
    copies = [
        pltpu.make_async_copy(src, dst, sem.at[n])
        for n, (src, dst) in enumerate(((gate_in, gate_hbm), (up_in, up_hbm), (down_in, down_hbm), (mixed, mixed_hbm)))
    ]
    for copy in copies[:3]:
        copy.start()
    ended = in_lanes(begun_ref[:, LANES:], mix_of(cmap, back_ref[...]))
    values = jnp.concatenate([begun_ref[:, :LANES], ended], axis=1).astype(BF16)
    a, b = iota((PART, PART), 0), iota((PART, PART), 1)
    order = jnp.where((a % 64) // DEPTH * 64 + a // 64 * DEPTH + a % DEPTH == b, 1.0, 0.0).astype(BF16)
    mixed[...] = jnp.dot(values, order, preferred_element_type=F32).astype(BF16)
    copies[3].start()
    for copy in copies:
        copy.wait()


def kernel(
    tok_hbm, routes_hbm, weight_hbm, gain_hbm, wg_hbm, wu_hbm, wd_hbm,
    gate_in, up_in, down_in, cmap, begun_ref, back_ref,
    routes_ref, weight_ref, gain_ref, tok, mine, normed, dest, gate_own, up_own, outgoing, rows, hidden,
    pair_out, pair_in, own, chip, relay, merged, ring_in, result, back,
    load_sem, self_sem, gu_send, gu_recv, dn_send, dn_recv, tok_send, tok_recv,
    y_send, y_recv, core_send, core_recv, pair_send, pair_recv, ring_send, ring_recv, back_send, back_recv,
):
    gr, fs, tp = lax.axis_index("gr"), lax.axis_index("fs"), lax.axis_index("tp")
    z, x = gr * 4 + fs // 4, fs % 4
    y, core = tp // 2, tp % 2
    me = gr * 16 + fs
    odd = z % 2

    def plane(z2, x2):
        return {"gr": z2 // 4, "fs": (z2 % 4) * 4 + x2, "tp": tp}

    def peer(k):
        i, turn = k // 4, k % 4
        far = (i + 1) // 2
        step = (i % 2) * far + (1 - i % 2) * ((8 - far) % 8)
        turn = (i % 2) * turn + (1 - i % 2) * ((4 - turn) % 4)
        return (z + step) % 8, (x + turn) % 4

    def column(y2, core2):
        return {"gr": gr, "fs": fs, "tp": y2 * 2 + core2}

    def remote(src, dst, send, recv, device):
        return pltpu.make_async_remote_copy(
            src_ref=src, dst_ref=dst, send_sem=send, recv_sem=recv, device_id=device, device_id_type=MESH
        )

    def drained(ref, sem):
        pltpu.make_async_copy(ref, ref, sem).wait()

    barrier = pltpu.get_barrier_semaphore()

    def greet(device):
        pl.semaphore_signal(barrier, inc=1, device_id=device, device_id_type=MESH)

    turns_x = [(x + turn) % 4 for turn in range(4)]
    for step in (4, 3, 5, 2, 6, 1, 7, 0):
        z2 = (z + step) % 8
        half, first = z2 // 4, z2 % 4 * 4
        for turn in (2, 1, 3, 0):
            if step + turn:
                greet({"gr": half, "fs": first + turns_x[turn], "tp": tp})
    for turn in (2, 1, 3):
        greet(column((y + turn) % 4, core))
    greet(column(y, 1 - core))

    loads = [
        pltpu.make_async_copy(src, dst, load_sem.at[n])
        for n, (src, dst) in enumerate(
            (
                (wg_hbm, gate_own),
                (wu_hbm, up_own),
                (tok_hbm, tok),
                (tok_hbm.at[:, pl.ds(pl.multiple_of(tp * PART, PART), PART)], mine),
                (routes_hbm, routes_ref),
                (weight_hbm, weight_ref),
                (gain_hbm, gain_ref),
            )
        )
    ]
    for load in (loads[6], *loads[:6]):
        load.start()

    loads[6].wait()
    diagonal = iota((64, 64), 0) == iota((64, 64), 1)
    gain = jnp.sum(jnp.where(diagonal, gain_ref[...], 0.0), axis=1, keepdims=True)
    loads[0].wait()
    loads[1].wait()

    def scale(e, carry):
        for ref in (gate_own, up_own):
            ref[e] = (ref[e].astype(F32) * gain).astype(BF16)
        return carry

    lax.fori_loop(0, EXPERTS, scale, 0)

    loads[4].wait()
    loads[5].wait()
    r0, r1 = routes_ref[0:1, :].astype(F32), routes_ref[1:2, :].astype(F32)
    names = iota((EXPERTS, TOK), 0).astype(F32)
    named = jnp.where((names == r0) | (names == r1), 1.0, 0.0)
    earlier = jnp.where(iota((TOK, TOK), 0) < iota((TOK, TOK), 1), 1.0, 0.0).astype(BF16)
    ranks = jnp.dot(named.astype(BF16), earlier, preferred_element_type=F32)
    for k, name in enumerate((r0, r1)):
        rank = jnp.sum(jnp.where(names == name, ranks, 0.0), axis=0, keepdims=True)
        dest[k : k + 1, :] = name * CAP + rank
        late = jnp.where(rank >= CAP // 2, float(PACKED - CAP // 2), 0.0)
        dest[2 + k : 3 + k, :] = name * (CAP // 2) + rank + late

    pl.semaphore_wait(barrier, 35)

    def send_gu(k, carry):
        z2, x2 = peer(k)
        e = (z2 % 4) * 4 + x2
        remote(gate_own.at[e], gate_in.at[me], gu_send.at[0], gu_recv.at[0], plane(z2, x2)).start()
        remote(up_own.at[e], up_in.at[me], gu_send.at[1], gu_recv.at[1], plane(z2, x2)).start()
        return carry

    lax.fori_loop(1, EARLY, send_gu, 0)

    loads[2].wait()
    loads[3].wait()

    def norm(b, carry):
        at = pl.ds(pl.multiple_of(b * 64, 64), 64)
        full = tok[at, :].astype(F32)
        inverse = lax.rsqrt(jnp.mean(full * full, axis=-1, keepdims=True) + EPSILON)
        normed[at, :] = (mine[at, :].astype(F32) * inverse).astype(BF16)
        return carry

    lax.fori_loop(0, TOK // 64, norm, 0)

    def pick(e, carry):
        slot = (iota((CAP, TOK), 0) + e * CAP).astype(F32)
        hits = jnp.where((slot == dest[0:1, :]) | (slot == dest[1:2, :]), 1.0, 0.0).astype(BF16)
        outgoing[e] = jnp.dot(hits, normed[...], preferred_element_type=F32).astype(BF16)
        return carry

    lax.fori_loop(0, EXPERTS, pick, 0)

    def slot_at(z2, z1):
        return (z1 - z2 + 2 - z2 % 2 + 16) % 8

    home = slot_at(z, z) * 4 + x

    def block(slot):
        return pl.ds(pl.multiple_of(slot * CAP, CAP), CAP)

    steps = [0, 1, 7, (1 - odd) * 2 + odd * 6]
    tok_self = pltpu.make_async_copy(outgoing.at[fs], rows.at[tp, block(home)], self_sem.at[0])
    tok_self.start()
    for i in range(4):
        for turn in range(4):
            if i + turn:
                z2, x2 = (z + steps[i]) % 8, (x + turn) % 4
                remote(
                    outgoing.at[(z2 % 4) * 4 + x2], rows.at[tp, block(slot_at(z2, z) * 4 + x)],
                    tok_send, tok_recv, plane(z2, x2),
                ).start()

    selves = [
        pltpu.make_async_copy(gate_own.at[fs], gate_in.at[me], self_sem.at[1]),
        pltpu.make_async_copy(up_own.at[fs], up_in.at[me], self_sem.at[2]),
        pltpu.make_async_copy(wd_hbm.at[fs], down_in.at[me], self_sem.at[3]),
    ]
    for copy in selves:
        copy.start()

    lax.fori_loop(EARLY, 32, send_gu, 0)

    def band(r):
        return pl.ds(pl.multiple_of(r * DEPTH, DEPTH), DEPTH)

    def send_dn(n, carry):
        r, k = n // 31, n % 31 + 1
        z2, x2 = peer(k)
        remote(
            wd_hbm.at[(z2 % 4) * 4 + x2, band(r)], down_in.at[me, band(r)],
            dn_send, dn_recv.at[r], plane(z2, x2),
        ).start()
        return carry

    lax.fori_loop(0, 31 * ROUNDS, send_dn, 0)

    across = iota((TOK, TOK), 0) == iota((TOK, TOK), 1)

    def upright(row):
        return jnp.sum(jnp.where(across, row, 0.0), axis=1, keepdims=True)

    mine_cols = jnp.concatenate(
        [upright(dest[2:3, :]), upright(dest[3:4, :]), upright(weight_ref[0:1, :]), upright(weight_ref[1:2, :])], axis=1
    )
    for b in range(8):
        cols = mine_cols[b * 64 : (b + 1) * 64]
        slot = iota((64, ROWS), 1).astype(F32)
        cmap[b * 64 : (b + 1) * 64, :] = (
            jnp.where(slot == cols[:, 0:1], cols[:, 2:3], 0.0) + jnp.where(slot == cols[:, 1:2], cols[:, 3:4], 0.0)
        ).astype(BF16)

    tok_self.wait()
    drained(outgoing.at[0:15], tok_recv)
    turns = (1, 3, 2)
    y_copies = [
        remote(rows.at[tp], rows.at[tp], y_send.at[turn - 1], y_recv.at[turn - 1], column((y + turn) % 4, core))
        for turn in turns
    ]
    for copy in y_copies:
        copy.start()
    core_copies = [remote(rows.at[tp], rows.at[tp], core_send.at[0], core_recv.at[0], column(y, 1 - core))]
    core_copies[0].start()
    for turn in turns:
        origin = ((y - turn + 4) % 4) * 2 + core
        drained(rows.at[origin], y_recv.at[turn - 1])
        core_copies.append(
            remote(rows.at[origin], rows.at[origin], core_send.at[turn], core_recv.at[turn], column(y, 1 - core))
        )
        core_copies[-1].start()
    for copy in core_copies:
        copy.wait_recv()

    for copy in selves:
        copy.wait()
    drained(gate_in.at[0:31], gu_recv.at[0])
    drained(up_in.at[0:31], gu_recv.at[1])

    def units(m, carry):
        at = pl.ds(pl.multiple_of(m * 4 * CAP, 4 * CAP), 4 * CAP)
        gate, upper = jnp.zeros((4 * CAP, UNITS), F32), jnp.zeros((4 * CAP, UNITS), F32)
        for j in range(TP):
            lhs = rows[j, at, :]
            gate += jnp.dot(lhs, gate_in[4 * j : 4 * j + 4].reshape(PART, UNITS), preferred_element_type=F32)
            upper += jnp.dot(lhs, up_in[4 * j : 4 * j + 4].reshape(PART, UNITS), preferred_element_type=F32)
        value = (gate / (1.0 + jnp.exp(-gate)) * upper).astype(BF16).reshape(4, 2, CAP // 2, UNITS)
        for half in range(2):
            hidden[half, pl.ds(4 * m, 4)] = value[:, half]
        return carry

    lax.fori_loop(0, EXPERTS // 4, units, 0)

    left = iota((8 * CAP // 2, LANES), 1) < LANES // 2
    pair_copies, ring_copies = [], []

    def half_block(slot):
        return pl.ds(pl.multiple_of(slot * (CAP // 2), CAP // 2), CAP // 2)

    def give_back(r):
        selves.append(pltpu.make_async_copy(result.at[r, half_block(home)], back.at[r, fs], self_sem.at[4 + r]))
        selves[-1].start()
        backs = [0, 1, 7, (1 - odd) * 6 + odd * 2]
        for i in (3, 1, 2, 0):
            for turn in range(4):
                if i + turn:
                    z1, x1 = (z + backs[i]) % 8, (x + turn) % 4
                    remote(
                        result.at[r, half_block(slot_at(z, z1) * 4 + x1)], back.at[r, fs],
                        back_send.at[r], back_recv.at[r], plane(z1, x1),
                    ).start()

    def sum_cores(r):
        drained(down_in.at[0:31, 0:DEPTH], dn_recv.at[r])

        def partial(parity, store):
            down = jnp.concatenate(
                [
                    down_in[pl.ds(4 * (2 * k + parity), 4), r * DEPTH : (r + 1) * DEPTH].reshape(4 * DEPTH, UNITS)
                    for k in range(4)
                ],
                axis=0,
            )

            for m in range(2):
                outs = [
                    lax.dot_general(
                        hidden[half, 8 * m : 8 * m + 8].reshape(4 * CAP, UNITS), down, (((1,), (1,)), ((), ())),
                        preferred_element_type=F32,
                    )
                    for half in range(2)
                ]
                for two in range(2):
                    lanes = slice(two * LANES, (two + 1) * LANES)
                    low, high = outs[0][:, lanes], outs[1][:, lanes]
                    at = slice(m * 4 * CAP, (m + 1) * 4 * CAP)
                    store(2 * two, at, jnp.where(left, low, pltpu.roll(high, LANES // 2, 1)))
                    store(2 * two + 1, at, jnp.where(left, pltpu.roll(low, LANES // 2, 1), high))

        def give(y2, at, value):
            pair_out[r, y2, at, :] = value.astype(BF16)

        def keep(y2, at, value):
            own[r, y2, at, :] = value

        partial(1 - core, give)
        for turn in (2, 1, 3, 0):
            y2 = (y + turn) % 4
            pair_copies.append(
                remote(
                    pair_out.at[r, y2], pair_in.at[r, y2], pair_send.at[r, y2], pair_recv.at[r, y2],
                    column(y, 1 - core),
                )
            )
            pair_copies[-1].start()
        partial(core, keep)
        low, high = slice(0, PACKED // 2), slice(PACKED // 2, PACKED)
        sides = ((0, (y + 1) % 4, low, high), (1, (y + 3) % 4, high, low))

        def ring(n, src, dst, device):
            ring_copies.append(remote(src, dst, ring_send.at[r, n], ring_recv.at[r, n], device))
            ring_copies[-1].start()

        for n, turn in enumerate((2, 1, 3, 0)):
            y2 = (y + turn) % 4
            pair_copies[4 * r + n].wait_recv()
            chip[r, y2] = (own[r, y2] + pair_in[r, y2].astype(F32)).astype(BF16)
            if turn == 2:
                for n, near, first, _ in sides:
                    ring(n, chip.at[r, y2, first], relay.at[r, n], column(near, core))
        for n, near, _, second in sides:
            ring(2 + n, chip.at[r, near, second], ring_in.at[r, n, second], column(near, core))
        if r == ROUNDS - 1:
            for before in range(r - 1):
                give_back(before)
        for n, near, first, _ in sides:
            ring_copies[6 * r + n].wait_recv()
            merged[r, n] = (chip[r, near, first].astype(F32) + relay[r, n].astype(F32)).astype(BF16)
            ring(4 + n, merged.at[r, n], ring_in.at[r, n, first], column(near, core))

    def sum_chips(r):
        for copy in ring_copies[6 * r + 2 : 6 * r + 6]:
            copy.wait_recv()
        value = chip[r, y].astype(F32)
        for n in range(2):
            value += ring_in[r, n].astype(F32)
        result[r] = value.astype(BF16)

    def mix(r):
        selves[3 + r].wait()
        drained(back.at[r, 0:15], back_recv.at[r])
        return mix_of(cmap, back[r])

    sum_cores(0)
    for r in range(1, ROUNDS):
        sum_cores(r)
        sum_chips(r - 1)
    give_back(ROUNDS - 2)
    sum_chips(ROUNDS - 1)
    give_back(ROUNDS - 1)
    begun_ref[:, :LANES] = in_lanes(mix(0), mix(1))
    begun_ref[:, LANES:] = mix(2)
    selves[6].wait()
    drained(back.at[3, 0:15], back_recv.at[3])
    back_ref[...] = back[3]

    drained(outgoing.at[0:15], tok_send)
    drained(gate_in.at[0:31], gu_send.at[0])
    drained(up_in.at[0:31], gu_send.at[1])
    drained(down_in.at[0:31], dn_send)
    for r in range(ROUNDS):
        drained(back.at[r, 0:15], back_send.at[r])
    for copy in y_copies + core_copies + pair_copies + ring_copies:
        copy.wait_send()


def body(tokens, routes, route_weight, gain, w_gate, w_up, w_down):
    anywhere = pl.BlockSpec(memory_space=pl.ANY)
    vmem = pl.BlockSpec(memory_space=pltpu.VMEM)
    weights = pltpu.VMEM((SOURCES, 64, UNITS), BF16)
    dma = pltpu.SemaphoreType.DMA
    held = pl.pallas_call(
        kernel,
        out_shape=(
            weights, weights, weights,
            pltpu.VMEM((TOK, ROWS), BF16),
            pltpu.VMEM((TOK, 2 * LANES), F32),
            pltpu.VMEM((EXPERTS, CAP // 2, LANES), BF16),
        ),
        in_specs=[anywhere] * 7,
        out_specs=(vmem,) * 6,
        scratch_shapes=[
            pltpu.VMEM((2, TOK), jnp.int32),
            pltpu.VMEM((2, TOK), F32),
            pltpu.VMEM((1, D // SOURCES), F32),
            pltpu.VMEM((TOK, D), BF16),
            pltpu.VMEM((TOK, PART), BF16),
            pltpu.VMEM((TOK, PART), BF16),
            pltpu.VMEM((4, TOK), F32),
            pltpu.VMEM((EXPERTS, 64, UNITS), BF16),
            pltpu.VMEM((EXPERTS, 64, UNITS), BF16),
            pltpu.VMEM((EXPERTS, CAP, PART), BF16),
            pltpu.VMEM((TP, ROWS, PART), BF16),
            pltpu.VMEM((2, EXPERTS, CAP // 2, UNITS), BF16),
            pltpu.VMEM((ROUNDS, 4, PACKED, LANES), BF16),
            pltpu.VMEM((ROUNDS, 4, PACKED, LANES), BF16),
            pltpu.VMEM((ROUNDS, 4, PACKED, LANES), F32),
            pltpu.VMEM((ROUNDS, 4, PACKED, LANES), BF16),
            pltpu.VMEM((ROUNDS, 2, PACKED // 2, LANES), BF16),
            pltpu.VMEM((ROUNDS, 2, PACKED // 2, LANES), BF16),
            pltpu.VMEM((ROUNDS, 2, PACKED, LANES), BF16),
            pltpu.VMEM((ROUNDS, PACKED, LANES), BF16),
            pltpu.VMEM((ROUNDS, EXPERTS, CAP // 2, LANES), BF16),
            dma((7,)),
            dma((8,)),
            dma((2,)), dma((2,)),
            dma, dma((ROUNDS,)),
            dma, dma,
            dma((3,)), dma((3,)),
            dma((4,)), dma((4,)),
            dma((ROUNDS, 4)), dma((ROUNDS, 4)),
            dma((ROUNDS, 6)), dma((ROUNDS, 6)),
            dma((ROUNDS,)), dma((ROUNDS,)),
        ],
        compiler_params=pltpu.CompilerParams(
            collective_id=0, has_side_effects=True, vmem_limit_bytes=48 * 1024 * 1024
        ),
    )(tokens, routes.T, route_weight.T, gain.reshape(1, -1), w_gate, w_up, w_down)
    placed = jax.ShapeDtypeStruct((SOURCES, 64, UNITS), BF16)
    gate_out, up_out, down_out, mixed = pl.pallas_call(
        finish,
        out_shape=(placed, placed, placed, jax.ShapeDtypeStruct((TOK, PART), BF16)),
        in_specs=[vmem] * 6,
        out_specs=(anywhere,) * 4,
        scratch_shapes=[pltpu.VMEM((TOK, PART), BF16), dma((4,))],
        compiler_params=pltpu.CompilerParams(vmem_limit_bytes=16 * 1024 * 1024),
    )(*held)
    return tuple(w.reshape(1, D, UNITS) for w in (gate_out, up_out, down_out)) + (mixed,)


def solution(mesh):
    rows = ("gr", "fs")
    weights = P(None, rows, "tp")
    placed = P("fs", None, "tp")
    return jax.shard_map(
        body,
        mesh=mesh,
        in_specs=(P(rows, None), P(rows, None), P(rows, None), P(rows), weights, weights, weights),
        out_specs=(placed, placed, placed, P(rows, "tp")),
        check_vma=False,
    )
```

```python
import functools

import jax
import jax.numpy as jnp
from jax import lax
from jax.experimental import pallas as pl
from jax.experimental.pallas import tpu as pltpu
from jax.sharding import PartitionSpec as P

MESH = pl.DeviceIdType.MESH
F32, BF16 = jnp.float32, jnp.bfloat16
EPSILON = 1e-05
D, UNITS, EXPERTS, TOK, CAP, TP, SOURCES = 2048, 512, 16, 512, 96, 8, 32
PART = D // TP
ROWS = EXPERTS * CAP
ROUNDS, DEPTH, LANES = 4, 16, 128
PACKED = ROWS // 2
EARLY = 12


def iota(shape, axis):
    return lax.broadcasted_iota(jnp.int32, shape, axis)


def mix_of(cmap, returned):
    returned = returned.reshape(PACKED, LANES)
    low = jnp.dot(cmap[:, :PACKED], returned, preferred_element_type=F32)
    high = jnp.dot(cmap[:, PACKED:], returned, preferred_element_type=F32)
    return low + pltpu.roll(high, LANES // 2, 1)


def in_lanes(one, other):
    first = iota((TOK, LANES), 1) < LANES // 2
    return jnp.where(first, one, pltpu.roll(other, LANES // 2, 1))


def finish(gate_in, up_in, down_in, cmap, begun_ref, back_ref, gate_hbm, up_hbm, down_hbm, mixed_hbm, mixed, sem):
    copies = [
        pltpu.make_async_copy(src, dst, sem.at[n])
        for n, (src, dst) in enumerate(((gate_in, gate_hbm), (up_in, up_hbm), (down_in, down_hbm), (mixed, mixed_hbm)))
    ]
    for copy in copies[:3]:
        copy.start()
    ended = in_lanes(begun_ref[:, LANES:], mix_of(cmap, back_ref[...]))
    values = jnp.concatenate([begun_ref[:, :LANES], ended], axis=1).astype(BF16)
    a, b = iota((PART, PART), 0), iota((PART, PART), 1)
    order = jnp.where((a % 64) // DEPTH * 64 + a // 64 * DEPTH + a % DEPTH == b, 1.0, 0.0).astype(BF16)
    mixed[...] = jnp.dot(values, order, preferred_element_type=F32).astype(BF16)
    copies[3].start()
    for copy in copies:
        copy.wait()


def kernel(
    tok_hbm, routes_hbm, weight_hbm, gain_hbm, wg_hbm, wu_hbm, wd_hbm,
    gate_in, up_in, down_in, cmap, begun_ref, back_ref,
    routes_ref, weight_ref, gain_ref, tok, mine, normed, dest, gate_own, up_own, down_own, outgoing, rows, hidden,
    pair_out, pair_in, own, chip, relay, merged, ring_in, result, back,
    load_sem, self_sem, gu_send, gu_recv, dn_send, dn_recv, tok_send, tok_recv,
    y_send, y_recv, core_send, core_recv, pair_send, pair_recv, ring_send, ring_recv, back_send, back_recv,
):
    gr, fs, tp = lax.axis_index("gr"), lax.axis_index("fs"), lax.axis_index("tp")
    z, x = gr * 4 + fs // 4, fs % 4
    y, core = tp // 2, tp % 2
    me = gr * 16 + fs
    odd = z % 2

    def plane(z2, x2):
        return {"gr": z2 // 4, "fs": (z2 % 4) * 4 + x2, "tp": tp}

    def peer(k):
        i, turn = k // 4, k % 4
        far = (i + 1) // 2
        step = (i % 2) * far + (1 - i % 2) * ((8 - far) % 8)
        turn = (i % 2) * turn + (1 - i % 2) * ((4 - turn) % 4)
        return (z + step) % 8, (x + turn) % 4

    def column(y2, core2):
        return {"gr": gr, "fs": fs, "tp": y2 * 2 + core2}

    def remote(src, dst, send, recv, device):
        return pltpu.make_async_remote_copy(
            src_ref=src, dst_ref=dst, send_sem=send, recv_sem=recv, device_id=device, device_id_type=MESH
        )

    def drained(ref, sem):
        pltpu.make_async_copy(ref, ref, sem).wait()

    barrier = pltpu.get_barrier_semaphore()

    def greet(device):
        pl.semaphore_signal(barrier, inc=1, device_id=device, device_id_type=MESH)

    turns_x = [(x + turn) % 4 for turn in range(4)]
    for step in (4, 3, 5, 2, 6, 1, 7, 0):
        z2 = (z + step) % 8
        half, first = z2 // 4, z2 % 4 * 4
        for turn in (2, 1, 3, 0):
            if step + turn:
                greet({"gr": half, "fs": first + turns_x[turn], "tp": tp})
    for turn in (2, 1, 3):
        greet(column((y + turn) % 4, core))
    greet(column(y, 1 - core))

    loads = [
        pltpu.make_async_copy(src, dst, load_sem.at[n])
        for n, (src, dst) in enumerate(
            (
                (wg_hbm, gate_own),
                (wu_hbm, up_own),
                (tok_hbm, tok),
                (tok_hbm.at[:, pl.ds(pl.multiple_of(tp * PART, PART), PART)], mine),
                (routes_hbm, routes_ref),
                (weight_hbm, weight_ref),
                (gain_hbm, gain_ref),
                (wd_hbm, down_own),
            )
        )
    ]
    for load in (loads[6], *loads[:6], loads[7]):
        load.start()

    loads[6].wait()
    diagonal = iota((64, 64), 0) == iota((64, 64), 1)
    gain = jnp.sum(jnp.where(diagonal, gain_ref[...], 0.0), axis=1, keepdims=True)
    loads[0].wait()
    loads[1].wait()

    def scale(e, carry):
        for ref in (gate_own, up_own):
            ref[e] = (ref[e].astype(F32) * gain).astype(BF16)
        return carry

    lax.fori_loop(0, EXPERTS, scale, 0)

    loads[4].wait()
    loads[5].wait()
    r0, r1 = routes_ref[0:1, :].astype(F32), routes_ref[1:2, :].astype(F32)
    names = iota((EXPERTS, TOK), 0).astype(F32)
    named = jnp.where((names == r0) | (names == r1), 1.0, 0.0)
    earlier = jnp.where(iota((TOK, TOK), 0) < iota((TOK, TOK), 1), 1.0, 0.0).astype(BF16)
    ranks = jnp.dot(named.astype(BF16), earlier, preferred_element_type=F32)
    for k, name in enumerate((r0, r1)):
        rank = jnp.sum(jnp.where(names == name, ranks, 0.0), axis=0, keepdims=True)
        dest[k : k + 1, :] = name * CAP + rank
        late = jnp.where(rank >= CAP // 2, float(PACKED - CAP // 2), 0.0)
        dest[2 + k : 3 + k, :] = name * (CAP // 2) + rank + late

    pl.semaphore_wait(barrier, 35)

    def send_gu(k, carry):
        z2, x2 = peer(k)
        e = (z2 % 4) * 4 + x2
        remote(gate_own.at[e], gate_in.at[me], gu_send.at[0], gu_recv.at[0], plane(z2, x2)).start()
        remote(up_own.at[e], up_in.at[me], gu_send.at[1], gu_recv.at[1], plane(z2, x2)).start()
        return carry

    lax.fori_loop(1, EARLY, send_gu, 0)

    loads[2].wait()
    loads[3].wait()

    def norm(b, carry):
        at = pl.ds(pl.multiple_of(b * 64, 64), 64)
        full = tok[at, :].astype(F32)
        inverse = lax.rsqrt(jnp.mean(full * full, axis=-1, keepdims=True) + EPSILON)
        normed[at, :] = (mine[at, :].astype(F32) * inverse).astype(BF16)
        return carry

    lax.fori_loop(0, TOK // 64, norm, 0)

    def pick(e, carry):
        slot = (iota((CAP, TOK), 0) + e * CAP).astype(F32)
        hits = jnp.where((slot == dest[0:1, :]) | (slot == dest[1:2, :]), 1.0, 0.0).astype(BF16)
        outgoing[e] = jnp.dot(hits, normed[...], preferred_element_type=F32).astype(BF16)
        return carry

    lax.fori_loop(0, EXPERTS, pick, 0)

    def slot_at(z2, z1):
        return (z1 - z2 + 2 - z2 % 2 + 16) % 8

    home = slot_at(z, z) * 4 + x

    def block(slot):
        return pl.ds(pl.multiple_of(slot * CAP, CAP), CAP)

    steps = [0, 1, 7, (1 - odd) * 2 + odd * 6]
    tok_self = pltpu.make_async_copy(outgoing.at[fs], rows.at[tp, block(home)], self_sem.at[0])
    tok_self.start()
    for i in range(4):
        for turn in range(4):
            if i + turn:
                z2, x2 = (z + steps[i]) % 8, (x + turn) % 4
                remote(
                    outgoing.at[(z2 % 4) * 4 + x2], rows.at[tp, block(slot_at(z2, z) * 4 + x)],
                    tok_send, tok_recv, plane(z2, x2),
                ).start()

    loads[7].wait()
    selves = [
        pltpu.make_async_copy(gate_own.at[fs], gate_in.at[me], self_sem.at[1]),
        pltpu.make_async_copy(up_own.at[fs], up_in.at[me], self_sem.at[2]),
        pltpu.make_async_copy(down_own.at[fs], down_in.at[me], self_sem.at[3]),
    ]
    for copy in selves:
        copy.start()

    lax.fori_loop(EARLY, 32, lambda k, carry: send_gu(31 + EARLY - k, carry), 0)

    def band(r):
        return pl.ds(pl.multiple_of(r * DEPTH, DEPTH), DEPTH)

    def send_dn(n, carry):
        r, k = n // 31, 31 - n % 31
        z2, x2 = peer(k)
        remote(
            down_own.at[(z2 % 4) * 4 + x2, band(r)], down_in.at[me, band(r)],
            dn_send, dn_recv.at[r], plane(z2, x2),
        ).start()
        return carry

    lax.fori_loop(0, 31 * ROUNDS, send_dn, 0)

    across = iota((TOK, TOK), 0) == iota((TOK, TOK), 1)

    def upright(row):
        return jnp.sum(jnp.where(across, row, 0.0), axis=1, keepdims=True)

    mine_cols = jnp.concatenate(
        [upright(dest[2:3, :]), upright(dest[3:4, :]), upright(weight_ref[0:1, :]), upright(weight_ref[1:2, :])], axis=1
    )
    for b in range(8):
        cols = mine_cols[b * 64 : (b + 1) * 64]
        slot = iota((64, ROWS), 1).astype(F32)
        cmap[b * 64 : (b + 1) * 64, :] = (
            jnp.where(slot == cols[:, 0:1], cols[:, 2:3], 0.0) + jnp.where(slot == cols[:, 1:2], cols[:, 3:4], 0.0)
        ).astype(BF16)

    tok_self.wait()
    drained(outgoing.at[0:15], tok_recv)
    turns = (1, 3, 2)
    y_copies = [
        remote(rows.at[tp], rows.at[tp], y_send.at[turn - 1], y_recv.at[turn - 1], column((y + turn) % 4, core))
        for turn in turns
    ]
    for copy in y_copies:
        copy.start()
    core_copies = [remote(rows.at[tp], rows.at[tp], core_send.at[0], core_recv.at[0], column(y, 1 - core))]
    core_copies[0].start()
    for turn in turns:
        origin = ((y - turn + 4) % 4) * 2 + core
        drained(rows.at[origin], y_recv.at[turn - 1])
        core_copies.append(
            remote(rows.at[origin], rows.at[origin], core_send.at[turn], core_recv.at[turn], column(y, 1 - core))
        )
        core_copies[-1].start()
    for copy in core_copies:
        copy.wait_recv()

    for copy in selves:
        copy.wait()
    drained(gate_in.at[0:31], gu_recv.at[0])
    drained(up_in.at[0:31], gu_recv.at[1])

    def units(m, carry):
        at = pl.ds(pl.multiple_of(m * 4 * CAP, 4 * CAP), 4 * CAP)
        gate, upper = jnp.zeros((4 * CAP, UNITS), F32), jnp.zeros((4 * CAP, UNITS), F32)
        for j in range(TP):
            lhs = rows[j, at, :]
            gate += jnp.dot(lhs, gate_in[4 * j : 4 * j + 4].reshape(PART, UNITS), preferred_element_type=F32)
            upper += jnp.dot(lhs, up_in[4 * j : 4 * j + 4].reshape(PART, UNITS), preferred_element_type=F32)
        value = (gate / (1.0 + jnp.exp(-gate)) * upper).astype(BF16).reshape(4, 2, CAP // 2, UNITS)
        for half in range(2):
            hidden[half, pl.ds(4 * m, 4)] = value[:, half]
        return carry

    lax.fori_loop(0, EXPERTS // 4, units, 0)

    left = iota((8 * CAP // 2, LANES), 1) < LANES // 2
    pair_copies, ring_copies = [], []

    def half_block(slot):
        return pl.ds(pl.multiple_of(slot * (CAP // 2), CAP // 2), CAP // 2)

    def give_back(r):
        selves.append(pltpu.make_async_copy(result.at[r, half_block(home)], back.at[r, fs], self_sem.at[4 + r]))
        selves[-1].start()
        backs = [0, 1, 7, (1 - odd) * 6 + odd * 2]
        for i in (3, 1, 2, 0):
            for turn in range(4):
                if i + turn:
                    z1, x1 = (z + backs[i]) % 8, (x + turn) % 4
                    remote(
                        result.at[r, half_block(slot_at(z, z1) * 4 + x1)], back.at[r, fs],
                        back_send.at[r], back_recv.at[r], plane(z1, x1),
                    ).start()

    def sum_cores(r):
        drained(down_in.at[0:31, 0:DEPTH], dn_recv.at[r])

        def partial(parity, store):
            down = jnp.concatenate(
                [
                    down_in[pl.ds(4 * (2 * k + parity), 4), r * DEPTH : (r + 1) * DEPTH].reshape(4 * DEPTH, UNITS)
                    for k in range(4)
                ],
                axis=0,
            )

            for m in range(2):
                outs = [
                    lax.dot_general(
                        hidden[half, 8 * m : 8 * m + 8].reshape(4 * CAP, UNITS), down, (((1,), (1,)), ((), ())),
                        preferred_element_type=F32,
                    )
                    for half in range(2)
                ]
                for two in range(2):
                    lanes = slice(two * LANES, (two + 1) * LANES)
                    low, high = outs[0][:, lanes], outs[1][:, lanes]
                    at = slice(m * 4 * CAP, (m + 1) * 4 * CAP)
                    store(2 * two, at, jnp.where(left, low, pltpu.roll(high, LANES // 2, 1)))
                    store(2 * two + 1, at, jnp.where(left, pltpu.roll(low, LANES // 2, 1), high))

        def give(y2, at, value):
            pair_out[r, y2, at, :] = value.astype(BF16)

        def keep(y2, at, value):
            own[r, y2, at, :] = value

        partial(1 - core, give)
        for turn in (2, 1, 3, 0):
            y2 = (y + turn) % 4
            pair_copies.append(
                remote(
                    pair_out.at[r, y2], pair_in.at[r, y2], pair_send.at[r, y2], pair_recv.at[r, y2],
                    column(y, 1 - core),
                )
            )
            pair_copies[-1].start()
        partial(core, keep)
        low, high = slice(0, PACKED // 2), slice(PACKED // 2, PACKED)
        sides = ((0, (y + 1) % 4, low, high), (1, (y + 3) % 4, high, low))

        def ring(n, src, dst, device):
            ring_copies.append(remote(src, dst, ring_send.at[r, n], ring_recv.at[r, n], device))
            ring_copies[-1].start()

        for n, turn in enumerate((2, 1, 3, 0)):
            y2 = (y + turn) % 4
            pair_copies[4 * r + n].wait_recv()
            chip[r, y2] = (own[r, y2] + pair_in[r, y2].astype(F32)).astype(BF16)
            if turn == 2:
                for n, near, first, _ in sides:
                    ring(n, chip.at[r, y2, first], relay.at[r, n], column(near, core))
        for n, near, _, second in sides:
            ring(2 + n, chip.at[r, near, second], ring_in.at[r, n, second], column(near, core))
        if r == ROUNDS - 1:
            for before in range(r - 1):
                give_back(before)
        for n, near, first, _ in sides:
            ring_copies[6 * r + n].wait_recv()
            merged[r, n] = (chip[r, near, first].astype(F32) + relay[r, n].astype(F32)).astype(BF16)
            ring(4 + n, merged.at[r, n], ring_in.at[r, n, first], column(near, core))

    def sum_chips(r):
        for copy in ring_copies[6 * r + 2 : 6 * r + 6]:
            copy.wait_recv()
        value = chip[r, y].astype(F32)
        for n in range(2):
            value += ring_in[r, n].astype(F32)
        result[r] = value.astype(BF16)

    def mix(r):
        selves[3 + r].wait()
        drained(back.at[r, 0:15], back_recv.at[r])
        return mix_of(cmap, back[r])

    sum_cores(0)
    for r in range(1, ROUNDS):
        sum_cores(r)
        sum_chips(r - 1)
    give_back(ROUNDS - 2)
    sum_chips(ROUNDS - 1)
    give_back(ROUNDS - 1)
    begun_ref[:, :LANES] = in_lanes(mix(0), mix(1))
    begun_ref[:, LANES:] = mix(2)
    selves[6].wait()
    drained(back.at[3, 0:15], back_recv.at[3])
    back_ref[...] = back[3]

    drained(outgoing.at[0:15], tok_send)
    drained(gate_in.at[0:31], gu_send.at[0])
    drained(up_in.at[0:31], gu_send.at[1])
    drained(down_in.at[0:31], dn_send)
    for r in range(ROUNDS):
        drained(back.at[r, 0:15], back_send.at[r])
    for copy in y_copies + core_copies + pair_copies + ring_copies:
        copy.wait_send()


def body(tokens, routes, route_weight, gain, w_gate, w_up, w_down):
    anywhere = pl.BlockSpec(memory_space=pl.ANY)
    vmem = pl.BlockSpec(memory_space=pltpu.VMEM)
    weights = pltpu.VMEM((SOURCES, 64, UNITS), BF16)
    dma = pltpu.SemaphoreType.DMA
    held = pl.pallas_call(
        kernel,
        out_shape=(
            weights, weights, weights,
            pltpu.VMEM((TOK, ROWS), BF16),
            pltpu.VMEM((TOK, 2 * LANES), F32),
            pltpu.VMEM((EXPERTS, CAP // 2, LANES), BF16),
        ),
        in_specs=[anywhere] * 7,
        out_specs=(vmem,) * 6,
        scratch_shapes=[
            pltpu.VMEM((2, TOK), jnp.int32),
            pltpu.VMEM((2, TOK), F32),
            pltpu.VMEM((1, D // SOURCES), F32),
            pltpu.VMEM((TOK, D), BF16),
            pltpu.VMEM((TOK, PART), BF16),
            pltpu.VMEM((TOK, PART), BF16),
            pltpu.VMEM((4, TOK), F32),
            pltpu.VMEM((EXPERTS, 64, UNITS), BF16),
            pltpu.VMEM((EXPERTS, 64, UNITS), BF16),
            pltpu.VMEM((EXPERTS, 64, UNITS), BF16),
            pltpu.VMEM((EXPERTS, CAP, PART), BF16),
            pltpu.VMEM((TP, ROWS, PART), BF16),
            pltpu.VMEM((2, EXPERTS, CAP // 2, UNITS), BF16),
            pltpu.VMEM((ROUNDS, 4, PACKED, LANES), BF16),
            pltpu.VMEM((ROUNDS, 4, PACKED, LANES), BF16),
            pltpu.VMEM((ROUNDS, 4, PACKED, LANES), F32),
            pltpu.VMEM((ROUNDS, 4, PACKED, LANES), BF16),
            pltpu.VMEM((ROUNDS, 2, PACKED // 2, LANES), BF16),
            pltpu.VMEM((ROUNDS, 2, PACKED // 2, LANES), BF16),
            pltpu.VMEM((ROUNDS, 2, PACKED, LANES), BF16),
            pltpu.VMEM((ROUNDS, PACKED, LANES), BF16),
            pltpu.VMEM((ROUNDS, EXPERTS, CAP // 2, LANES), BF16),
            dma((8,)),
            dma((8,)),
            dma((2,)), dma((2,)),
            dma, dma((ROUNDS,)),
            dma, dma,
            dma((3,)), dma((3,)),
            dma((4,)), dma((4,)),
            dma((ROUNDS, 4)), dma((ROUNDS, 4)),
            dma((ROUNDS, 6)), dma((ROUNDS, 6)),
            dma((ROUNDS,)), dma((ROUNDS,)),
        ],
        compiler_params=pltpu.CompilerParams(
            collective_id=0, has_side_effects=True, vmem_limit_bytes=48 * 1024 * 1024
        ),
    )(tokens, routes.T, route_weight.T, gain.reshape(1, -1), w_gate, w_up, w_down)
    placed = jax.ShapeDtypeStruct((SOURCES, 64, UNITS), BF16)
    gate_out, up_out, down_out, mixed = pl.pallas_call(
        finish,
        out_shape=(placed, placed, placed, jax.ShapeDtypeStruct((TOK, PART), BF16)),
        in_specs=[vmem] * 6,
        out_specs=(anywhere,) * 4,
        scratch_shapes=[pltpu.VMEM((TOK, PART), BF16), dma((4,))],
        compiler_params=pltpu.CompilerParams(vmem_limit_bytes=16 * 1024 * 1024),
    )(*held)
    return tuple(w.reshape(1, D, UNITS) for w in (gate_out, up_out, down_out)) + (mixed,)


def solution(mesh):
    rows = ("gr", "fs")
    weights = P(None, rows, "tp")
    placed = P("fs", None, "tp")
    return jax.shard_map(
        body,
        mesh=mesh,
        in_specs=(P(rows, None), P(rows, None), P(rows, None), P(rows), weights, weights, weights),
        out_specs=(placed, placed, placed, P(rows, "tp")),
        check_vma=False,
    )
```

```python
import functools

import jax
import jax.numpy as jnp
from jax import lax
from jax.experimental import pallas as pl
from jax.experimental.pallas import tpu as pltpu
from jax.sharding import PartitionSpec as P

MESH = pl.DeviceIdType.MESH
F32, BF16 = jnp.float32, jnp.bfloat16
EPSILON = 1e-05
D, UNITS, EXPERTS, TOK, CAP, TP, SOURCES = 2048, 512, 16, 512, 96, 8, 32
PART = D // TP
ROWS = EXPERTS * CAP
ROUNDS, DEPTH, LANES = 4, 16, 128
PACKED = ROWS // 2
EARLY = 12


def iota(shape, axis):
    return lax.broadcasted_iota(jnp.int32, shape, axis)


def mix_of(cmap, returned):
    returned = returned.reshape(PACKED, LANES)
    low = jnp.dot(cmap[:, :PACKED], returned, preferred_element_type=F32)
    high = jnp.dot(cmap[:, PACKED:], returned, preferred_element_type=F32)
    return low + pltpu.roll(high, LANES // 2, 1)


def in_lanes(one, other):
    first = iota((TOK, LANES), 1) < LANES // 2
    return jnp.where(first, one, pltpu.roll(other, LANES // 2, 1))


def finish(gate_in, up_in, down_in, cmap, begun_ref, back_ref, gate_hbm, up_hbm, down_hbm, mixed_hbm, mixed, sem):
    copies = [
        pltpu.make_async_copy(src, dst, sem.at[n])
        for n, (src, dst) in enumerate(((gate_in, gate_hbm), (up_in, up_hbm), (down_in, down_hbm), (mixed, mixed_hbm)))
    ]
    for copy in copies[:3]:
        copy.start()
    ended = in_lanes(begun_ref[:, LANES:], mix_of(cmap, back_ref[...]))
    values = jnp.concatenate([begun_ref[:, :LANES], ended], axis=1).astype(BF16)
    a, b = iota((PART, PART), 0), iota((PART, PART), 1)
    order = jnp.where((a % 64) // DEPTH * 64 + a // 64 * DEPTH + a % DEPTH == b, 1.0, 0.0).astype(BF16)
    mixed[...] = jnp.dot(values, order, preferred_element_type=F32).astype(BF16)
    copies[3].start()
    for copy in copies:
        copy.wait()


def kernel(
    tok_hbm, routes_hbm, weight_hbm, gain_hbm, wg_hbm, wu_hbm, wd_hbm,
    gate_in, up_in, down_in, cmap, begun_ref, back_ref,
    routes_ref, weight_ref, gain_ref, tok, mine, normed, dest, gate_own, up_own, down_own, outgoing, rows, hidden,
    pair_out, pair_in, own, chip, relay, merged, ring_in, result, back,
    load_sem, wave_sem, self_sem, gu_send, gu_recv, dn_send, dn_recv, tok_send, tok_recv,
    y_send, y_recv, core_send, core_recv, pair_send, pair_recv, ring_send, ring_recv, back_send, back_recv,
):
    gr, fs, tp = lax.axis_index("gr"), lax.axis_index("fs"), lax.axis_index("tp")
    z, x = gr * 4 + fs // 4, fs % 4
    y, core = tp // 2, tp % 2
    me = gr * 16 + fs
    odd = z % 2

    def plane(z2, x2):
        return {"gr": z2 // 4, "fs": (z2 % 4) * 4 + x2, "tp": tp}

    def peer(k):
        i, turn = k // 4, k % 4
        far = (i + 1) // 2
        step = (i % 2) * far + (1 - i % 2) * ((8 - far) % 8)
        turn = (i % 2) * turn + (1 - i % 2) * ((4 - turn) % 4)
        return (z + step) % 8, (x + turn) % 4

    def column(y2, core2):
        return {"gr": gr, "fs": fs, "tp": y2 * 2 + core2}

    def remote(src, dst, send, recv, device):
        return pltpu.make_async_remote_copy(
            src_ref=src, dst_ref=dst, send_sem=send, recv_sem=recv, device_id=device, device_id_type=MESH
        )

    def drained(ref, sem):
        pltpu.make_async_copy(ref, ref, sem).wait()

    barrier = pltpu.get_barrier_semaphore()

    def greet(device):
        pl.semaphore_signal(barrier, inc=1, device_id=device, device_id_type=MESH)

    turns_x = [(x + turn) % 4 for turn in range(4)]
    for step in (1, 7, 0):
        z2 = (z + step) % 8
        half, first = z2 // 4, z2 % 4 * 4
        for turn in (2, 1, 3, 0):
            if step + turn:
                greet({"gr": half, "fs": first + turns_x[turn], "tp": tp})
    for turn in (2, 1, 3):
        greet(column((y + turn) % 4, core))
    greet(column(y, 1 - core))

    loads = [
        pltpu.make_async_copy(src, dst, load_sem.at[n])
        for n, (src, dst) in enumerate(
            (
                (wg_hbm, gate_own),
                (wu_hbm, up_own),
                (tok_hbm, tok),
                (tok_hbm.at[:, pl.ds(pl.multiple_of(tp * PART, PART), PART)], mine),
                (routes_hbm, routes_ref),
                (weight_hbm, weight_ref),
                (gain_hbm, gain_ref),
                (wd_hbm, down_own),
            )
        )
    ]
    for load in (loads[6], *loads[:6], loads[7]):
        load.start()

    loads[6].wait()
    diagonal = iota((64, 64), 0) == iota((64, 64), 1)
    gain = jnp.sum(jnp.where(diagonal, gain_ref[...], 0.0), axis=1, keepdims=True)
    loads[0].wait()
    loads[1].wait()

    def scale(e, carry):
        for ref in (gate_own, up_own):
            ref[e] = (ref[e].astype(F32) * gain).astype(BF16)
        return carry

    lax.fori_loop(0, EXPERTS, scale, 0)

    pl.semaphore_wait(barrier, 15)

    def send_gu(k, carry):
        z2, x2 = peer(k)
        e = (z2 % 4) * 4 + x2
        remote(gate_own.at[e], gate_in.at[me], gu_send.at[0], gu_recv.at[0], plane(z2, x2)).start()
        remote(up_own.at[e], up_in.at[me], gu_send.at[1], gu_recv.at[1], plane(z2, x2)).start()
        return carry

    lax.fori_loop(1, EARLY, send_gu, 0)

    def hail(n):
        for side, step in ((0, 1), (1, 7)):
            pl.semaphore_signal(
                wave_sem.at[n, side], inc=1, device_id=plane((z + step) % 8, x), device_id_type=MESH
            )

    def heard(n):
        for side in range(2):
            pl.semaphore_wait(wave_sem.at[n, side], 1)

    hail(0)

    loads[4].wait()
    loads[5].wait()
    r0, r1 = routes_ref[0:1, :].astype(F32), routes_ref[1:2, :].astype(F32)
    names = iota((EXPERTS, TOK), 0).astype(F32)
    named = jnp.where((names == r0) | (names == r1), 1.0, 0.0)
    earlier = jnp.where(iota((TOK, TOK), 0) < iota((TOK, TOK), 1), 1.0, 0.0).astype(BF16)
    ranks = jnp.dot(named.astype(BF16), earlier, preferred_element_type=F32)
    for k, name in enumerate((r0, r1)):
        rank = jnp.sum(jnp.where(names == name, ranks, 0.0), axis=0, keepdims=True)
        dest[k : k + 1, :] = name * CAP + rank
        late = jnp.where(rank >= CAP // 2, float(PACKED - CAP // 2), 0.0)
        dest[2 + k : 3 + k, :] = name * (CAP // 2) + rank + late

    loads[2].wait()
    loads[3].wait()

    def norm(b, carry):
        at = pl.ds(pl.multiple_of(b * 64, 64), 64)
        full = tok[at, :].astype(F32)
        inverse = lax.rsqrt(jnp.mean(full * full, axis=-1, keepdims=True) + EPSILON)
        normed[at, :] = (mine[at, :].astype(F32) * inverse).astype(BF16)
        return carry

    lax.fori_loop(0, TOK // 64, norm, 0)
    heard(0)
    hail(1)

    def pick(e, carry):
        slot = (iota((CAP, TOK), 0) + e * CAP).astype(F32)
        hits = jnp.where((slot == dest[0:1, :]) | (slot == dest[1:2, :]), 1.0, 0.0).astype(BF16)
        outgoing[e] = jnp.dot(hits, normed[...], preferred_element_type=F32).astype(BF16)
        return carry

    lax.fori_loop(0, EXPERTS, pick, 0)
    heard(1)
    hail(2)

    def slot_at(z2, z1):
        return (z1 - z2 + 2 - z2 % 2 + 16) % 8

    home = slot_at(z, z) * 4 + x

    def block(slot):
        return pl.ds(pl.multiple_of(slot * CAP, CAP), CAP)

    steps = [0, 1, 7, (1 - odd) * 2 + odd * 6]
    tok_self = pltpu.make_async_copy(outgoing.at[fs], rows.at[tp, block(home)], self_sem.at[0])
    tok_self.start()
    for i in range(4):
        for turn in range(4):
            if i + turn:
                z2, x2 = (z + steps[i]) % 8, (x + turn) % 4
                remote(
                    outgoing.at[(z2 % 4) * 4 + x2], rows.at[tp, block(slot_at(z2, z) * 4 + x)],
                    tok_send, tok_recv, plane(z2, x2),
                ).start()

    loads[7].wait()
    selves = [
        pltpu.make_async_copy(gate_own.at[fs], gate_in.at[me], self_sem.at[1]),
        pltpu.make_async_copy(up_own.at[fs], up_in.at[me], self_sem.at[2]),
        pltpu.make_async_copy(down_own.at[fs], down_in.at[me], self_sem.at[3]),
    ]
    for copy in selves:
        copy.start()

    heard(2)
    lax.fori_loop(EARLY, 32, lambda k, carry: send_gu(31 + EARLY - k, carry), 0)

    def band(r):
        return pl.ds(pl.multiple_of(r * DEPTH, DEPTH), DEPTH)

    def send_dn(n, carry):
        r, k = n // 31, 31 - n % 31
        z2, x2 = peer(k)
        remote(
            down_own.at[(z2 % 4) * 4 + x2, band(r)], down_in.at[me, band(r)],
            dn_send, dn_recv.at[r], plane(z2, x2),
        ).start()
        return carry

    lax.fori_loop(0, 31 * ROUNDS, send_dn, 0)

    across = iota((TOK, TOK), 0) == iota((TOK, TOK), 1)

    def upright(row):
        return jnp.sum(jnp.where(across, row, 0.0), axis=1, keepdims=True)

    mine_cols = jnp.concatenate(
        [upright(dest[2:3, :]), upright(dest[3:4, :]), upright(weight_ref[0:1, :]), upright(weight_ref[1:2, :])], axis=1
    )
    for b in range(8):
        cols = mine_cols[b * 64 : (b + 1) * 64]
        slot = iota((64, ROWS), 1).astype(F32)
        cmap[b * 64 : (b + 1) * 64, :] = (
            jnp.where(slot == cols[:, 0:1], cols[:, 2:3], 0.0) + jnp.where(slot == cols[:, 1:2], cols[:, 3:4], 0.0)
        ).astype(BF16)

    tok_self.wait()
    drained(outgoing.at[0:15], tok_recv)
    turns = (1, 3, 2)
    y_copies = [
        remote(rows.at[tp], rows.at[tp], y_send.at[turn - 1], y_recv.at[turn - 1], column((y + turn) % 4, core))
        for turn in turns
    ]
    for copy in y_copies:
        copy.start()
    core_copies = [remote(rows.at[tp], rows.at[tp], core_send.at[0], core_recv.at[0], column(y, 1 - core))]
    core_copies[0].start()
    for turn in turns:
        origin = ((y - turn + 4) % 4) * 2 + core
        drained(rows.at[origin], y_recv.at[turn - 1])
        core_copies.append(
            remote(rows.at[origin], rows.at[origin], core_send.at[turn], core_recv.at[turn], column(y, 1 - core))
        )
        core_copies[-1].start()
    for copy in core_copies:
        copy.wait_recv()

    for copy in selves:
        copy.wait()
    drained(gate_in.at[0:31], gu_recv.at[0])
    drained(up_in.at[0:31], gu_recv.at[1])

    def units(m, carry):
        at = pl.ds(pl.multiple_of(m * 4 * CAP, 4 * CAP), 4 * CAP)
        gate, upper = jnp.zeros((4 * CAP, UNITS), F32), jnp.zeros((4 * CAP, UNITS), F32)
        for j in range(TP):
            lhs = rows[j, at, :]
            gate += jnp.dot(lhs, gate_in[4 * j : 4 * j + 4].reshape(PART, UNITS), preferred_element_type=F32)
            upper += jnp.dot(lhs, up_in[4 * j : 4 * j + 4].reshape(PART, UNITS), preferred_element_type=F32)
        value = (gate / (1.0 + jnp.exp(-gate)) * upper).astype(BF16).reshape(4, 2, CAP // 2, UNITS)
        for half in range(2):
            hidden[half, pl.ds(4 * m, 4)] = value[:, half]
        return carry

    lax.fori_loop(0, EXPERTS // 4, units, 0)

    left = iota((8 * CAP // 2, LANES), 1) < LANES // 2
    pair_copies, ring_copies = [], []

    def half_block(slot):
        return pl.ds(pl.multiple_of(slot * (CAP // 2), CAP // 2), CAP // 2)

    def give_back(r):
        selves.append(pltpu.make_async_copy(result.at[r, half_block(home)], back.at[r, fs], self_sem.at[4 + r]))
        selves[-1].start()
        backs = [0, 1, 7, (1 - odd) * 6 + odd * 2]
        for i in (3, 1, 2, 0):
            for turn in range(4):
                if i + turn:
                    z1, x1 = (z + backs[i]) % 8, (x + turn) % 4
                    remote(
                        result.at[r, half_block(slot_at(z, z1) * 4 + x1)], back.at[r, fs],
                        back_send.at[r], back_recv.at[r], plane(z1, x1),
                    ).start()

    def sum_cores(r):
        drained(down_in.at[0:31, 0:DEPTH], dn_recv.at[r])

        def partial(parity, store):
            down = jnp.concatenate(
                [
                    down_in[pl.ds(4 * (2 * k + parity), 4), r * DEPTH : (r + 1) * DEPTH].reshape(4 * DEPTH, UNITS)
                    for k in range(4)
                ],
                axis=0,
            )

            for m in range(2):
                outs = [
                    lax.dot_general(
                        hidden[half, 8 * m : 8 * m + 8].reshape(4 * CAP, UNITS), down, (((1,), (1,)), ((), ())),
                        preferred_element_type=F32,
                    )
                    for half in range(2)
                ]
                for two in range(2):
                    lanes = slice(two * LANES, (two + 1) * LANES)
                    low, high = outs[0][:, lanes], outs[1][:, lanes]
                    at = slice(m * 4 * CAP, (m + 1) * 4 * CAP)
                    store(2 * two, at, jnp.where(left, low, pltpu.roll(high, LANES // 2, 1)))
                    store(2 * two + 1, at, jnp.where(left, pltpu.roll(low, LANES // 2, 1), high))

        def give(y2, at, value):
            pair_out[r, y2, at, :] = value.astype(BF16)

        def keep(y2, at, value):
            own[r, y2, at, :] = value

        partial(1 - core, give)
        for turn in (2, 1, 3, 0):
            y2 = (y + turn) % 4
            pair_copies.append(
                remote(
                    pair_out.at[r, y2], pair_in.at[r, y2], pair_send.at[r, y2], pair_recv.at[r, y2],
                    column(y, 1 - core),
                )
            )
            pair_copies[-1].start()
        partial(core, keep)
        low, high = slice(0, PACKED // 2), slice(PACKED // 2, PACKED)
        sides = ((0, (y + 1) % 4, low, high), (1, (y + 3) % 4, high, low))

        def ring(n, src, dst, device):
            ring_copies.append(remote(src, dst, ring_send.at[r, n], ring_recv.at[r, n], device))
            ring_copies[-1].start()

        for n, turn in enumerate((2, 1, 3, 0)):
            y2 = (y + turn) % 4
            pair_copies[4 * r + n].wait_recv()
            chip[r, y2] = (own[r, y2] + pair_in[r, y2].astype(F32)).astype(BF16)
            if turn == 2:
                for n, near, first, _ in sides:
                    ring(n, chip.at[r, y2, first], relay.at[r, n], column(near, core))
        for n, near, _, second in sides:
            ring(2 + n, chip.at[r, near, second], ring_in.at[r, n, second], column(near, core))
        if r == ROUNDS - 1:
            for before in range(r - 1):
                give_back(before)
        for n, near, first, _ in sides:
            ring_copies[6 * r + n].wait_recv()
            merged[r, n] = (chip[r, near, first].astype(F32) + relay[r, n].astype(F32)).astype(BF16)
            ring(4 + n, merged.at[r, n], ring_in.at[r, n, first], column(near, core))

    def sum_chips(r):
        for copy in ring_copies[6 * r + 2 : 6 * r + 6]:
            copy.wait_recv()
        value = chip[r, y].astype(F32)
        for n in range(2):
            value += ring_in[r, n].astype(F32)
        result[r] = value.astype(BF16)

    def mix(r):
        selves[3 + r].wait()
        drained(back.at[r, 0:15], back_recv.at[r])
        return mix_of(cmap, back[r])

    sum_cores(0)
    for r in range(1, ROUNDS):
        sum_cores(r)
        sum_chips(r - 1)
    give_back(ROUNDS - 2)
    sum_chips(ROUNDS - 1)
    give_back(ROUNDS - 1)
    begun_ref[:, :LANES] = in_lanes(mix(0), mix(1))
    begun_ref[:, LANES:] = mix(2)
    selves[6].wait()
    drained(back.at[3, 0:15], back_recv.at[3])
    back_ref[...] = back[3]

    drained(outgoing.at[0:15], tok_send)
    drained(gate_in.at[0:31], gu_send.at[0])
    drained(up_in.at[0:31], gu_send.at[1])
    drained(down_in.at[0:31], dn_send)
    for r in range(ROUNDS):
        drained(back.at[r, 0:15], back_send.at[r])
    for copy in y_copies + core_copies + pair_copies + ring_copies:
        copy.wait_send()


def body(tokens, routes, route_weight, gain, w_gate, w_up, w_down):
    anywhere = pl.BlockSpec(memory_space=pl.ANY)
    vmem = pl.BlockSpec(memory_space=pltpu.VMEM)
    weights = pltpu.VMEM((SOURCES, 64, UNITS), BF16)
    dma = pltpu.SemaphoreType.DMA
    held = pl.pallas_call(
        kernel,
        out_shape=(
            weights, weights, weights,
            pltpu.VMEM((TOK, ROWS), BF16),
            pltpu.VMEM((TOK, 2 * LANES), F32),
            pltpu.VMEM((EXPERTS, CAP // 2, LANES), BF16),
        ),
        in_specs=[anywhere] * 7,
        out_specs=(vmem,) * 6,
        scratch_shapes=[
            pltpu.VMEM((2, TOK), jnp.int32),
            pltpu.VMEM((2, TOK), F32),
            pltpu.VMEM((1, D // SOURCES), F32),
            pltpu.VMEM((TOK, D), BF16),
            pltpu.VMEM((TOK, PART), BF16),
            pltpu.VMEM((TOK, PART), BF16),
            pltpu.VMEM((4, TOK), F32),
            pltpu.VMEM((EXPERTS, 64, UNITS), BF16),
            pltpu.VMEM((EXPERTS, 64, UNITS), BF16),
            pltpu.VMEM((EXPERTS, 64, UNITS), BF16),
            pltpu.VMEM((EXPERTS, CAP, PART), BF16),
            pltpu.VMEM((TP, ROWS, PART), BF16),
            pltpu.VMEM((2, EXPERTS, CAP // 2, UNITS), BF16),
            pltpu.VMEM((ROUNDS, 4, PACKED, LANES), BF16),
            pltpu.VMEM((ROUNDS, 4, PACKED, LANES), BF16),
            pltpu.VMEM((ROUNDS, 4, PACKED, LANES), F32),
            pltpu.VMEM((ROUNDS, 4, PACKED, LANES), BF16),
            pltpu.VMEM((ROUNDS, 2, PACKED // 2, LANES), BF16),
            pltpu.VMEM((ROUNDS, 2, PACKED // 2, LANES), BF16),
            pltpu.VMEM((ROUNDS, 2, PACKED, LANES), BF16),
            pltpu.VMEM((ROUNDS, PACKED, LANES), BF16),
            pltpu.VMEM((ROUNDS, EXPERTS, CAP // 2, LANES), BF16),
            dma((8,)),
            pltpu.SemaphoreType.REGULAR((3, 2)),
            dma((8,)),
            dma((2,)), dma((2,)),
            dma, dma((ROUNDS,)),
            dma, dma,
            dma((3,)), dma((3,)),
            dma((4,)), dma((4,)),
            dma((ROUNDS, 4)), dma((ROUNDS, 4)),
            dma((ROUNDS, 6)), dma((ROUNDS, 6)),
            dma((ROUNDS,)), dma((ROUNDS,)),
        ],
        compiler_params=pltpu.CompilerParams(
            collective_id=0, has_side_effects=True, vmem_limit_bytes=48 * 1024 * 1024
        ),
    )(tokens, routes.T, route_weight.T, gain.reshape(1, -1), w_gate, w_up, w_down)
    placed = jax.ShapeDtypeStruct((SOURCES, 64, UNITS), BF16)
    gate_out, up_out, down_out, mixed = pl.pallas_call(
        finish,
        out_shape=(placed, placed, placed, jax.ShapeDtypeStruct((TOK, PART), BF16)),
        in_specs=[vmem] * 6,
        out_specs=(anywhere,) * 4,
        scratch_shapes=[pltpu.VMEM((TOK, PART), BF16), dma((4,))],
        compiler_params=pltpu.CompilerParams(vmem_limit_bytes=16 * 1024 * 1024),
    )(*held)
    return tuple(w.reshape(1, D, UNITS) for w in (gate_out, up_out, down_out)) + (mixed,)


def solution(mesh):
    rows = ("gr", "fs")
    weights = P(None, rows, "tp")
    placed = P("fs", None, "tp")
    return jax.shard_map(
        body,
        mesh=mesh,
        in_specs=(P(rows, None), P(rows, None), P(rows, None), P(rows), weights, weights, weights),
        out_specs=(placed, placed, placed, P(rows, "tp")),
        check_vma=False,
    )
```

```python
import functools

import jax
import jax.numpy as jnp
from jax import lax
from jax.experimental import pallas as pl
from jax.experimental.pallas import tpu as pltpu
from jax.sharding import PartitionSpec as P

MESH = pl.DeviceIdType.MESH
F32, BF16 = jnp.float32, jnp.bfloat16
EPSILON = 1e-05
D, UNITS, EXPERTS, TOK, CAP, TP, SOURCES = 2048, 512, 16, 512, 96, 8, 32
PART = D // TP
ROWS = EXPERTS * CAP
ROUNDS, DEPTH, LANES = 4, 16, 128
PACKED = ROWS // 2
EARLY = 12


def iota(shape, axis):
    return lax.broadcasted_iota(jnp.int32, shape, axis)


def mix_of(cmap, returned):
    returned = returned.reshape(PACKED, LANES)
    low = jnp.dot(cmap[:, :PACKED], returned, preferred_element_type=F32)
    high = jnp.dot(cmap[:, PACKED:], returned, preferred_element_type=F32)
    return low + pltpu.roll(high, LANES // 2, 1)


def in_lanes(one, other):
    first = iota((TOK, LANES), 1) < LANES // 2
    return jnp.where(first, one, pltpu.roll(other, LANES // 2, 1))


def finish(gate_in, up_in, down_in, cmap, begun_ref, back_ref, gate_hbm, up_hbm, down_hbm, mixed_hbm, mixed, sem):
    copies = [
        pltpu.make_async_copy(src, dst, sem.at[n])
        for n, (src, dst) in enumerate(((gate_in, gate_hbm), (up_in, up_hbm), (down_in, down_hbm), (mixed, mixed_hbm)))
    ]
    for copy in copies[:3]:
        copy.start()
    ended = in_lanes(begun_ref[:, LANES:], mix_of(cmap, back_ref[...]))
    values = jnp.concatenate([begun_ref[:, :LANES], ended], axis=1).astype(BF16)
    a, b = iota((PART, PART), 0), iota((PART, PART), 1)
    order = jnp.where((a % 64) // DEPTH * 64 + a // 64 * DEPTH + a % DEPTH == b, 1.0, 0.0).astype(BF16)
    mixed[...] = jnp.dot(values, order, preferred_element_type=F32).astype(BF16)
    copies[3].start()
    for copy in copies:
        copy.wait()


def kernel(
    tok_hbm, routes_hbm, weight_hbm, gain_hbm, wg_hbm, wu_hbm, wd_hbm,
    gate_in, up_in, down_in, cmap, begun_ref, back_ref,
    routes_ref, weight_ref, gain_ref, tok, mine, normed, dest, gate_own, up_own, down_own, outgoing, rows, hidden,
    pair_out, pair_in, own, chip, relay, merged, ring_in, result, back,
    load_sem, wave_sem, self_sem, gu_send, gu_recv, dn_send, dn_recv, tok_send, tok_recv,
    y_send, y_recv, core_send, core_recv, pair_send, pair_recv, ring_send, ring_recv, back_send, back_recv,
):
    gr, fs, tp = lax.axis_index("gr"), lax.axis_index("fs"), lax.axis_index("tp")
    z, x = gr * 4 + fs // 4, fs % 4
    y, core = tp // 2, tp % 2
    me = gr * 16 + fs
    odd = z % 2

    def plane(z2, x2):
        return {"gr": z2 // 4, "fs": (z2 % 4) * 4 + x2, "tp": tp}

    def peer(k):
        i, turn = k // 4, k % 4
        far = (i + 1) // 2
        step = (i % 2) * far + (1 - i % 2) * ((8 - far) % 8)
        turn = (i % 2) * turn + (1 - i % 2) * ((4 - turn) % 4)
        return (z + step) % 8, (x + turn) % 4

    def column(y2, core2):
        return {"gr": gr, "fs": fs, "tp": y2 * 2 + core2}

    def remote(src, dst, send, recv, device):
        return pltpu.make_async_remote_copy(
            src_ref=src, dst_ref=dst, send_sem=send, recv_sem=recv, device_id=device, device_id_type=MESH
        )

    def drained(ref, sem):
        pltpu.make_async_copy(ref, ref, sem).wait()

    barrier = pltpu.get_barrier_semaphore()

    def greet(device):
        pl.semaphore_signal(barrier, inc=1, device_id=device, device_id_type=MESH)

    turns_x = [(x + turn) % 4 for turn in range(4)]
    for step in (1, 7, 0):
        z2 = (z + step) % 8
        half, first = z2 // 4, z2 % 4 * 4
        for turn in (2, 1, 3, 0):
            if step + turn:
                greet({"gr": half, "fs": first + turns_x[turn], "tp": tp})
    for turn in (2, 1, 3):
        greet(column((y + turn) % 4, core))
    greet(column(y, 1 - core))

    loads = [
        pltpu.make_async_copy(src, dst, load_sem.at[n])
        for n, (src, dst) in enumerate(
            (
                (wg_hbm, gate_own),
                (wu_hbm, up_own),
                (tok_hbm, tok),
                (tok_hbm.at[:, pl.ds(pl.multiple_of(tp * PART, PART), PART)], mine),
                (routes_hbm, routes_ref),
                (weight_hbm, weight_ref),
                (gain_hbm, gain_ref),
                (wd_hbm, down_own),
            )
        )
    ]
    for load in (loads[6], *loads[:6], loads[7]):
        load.start()

    loads[6].wait()
    diagonal = iota((64, 64), 0) == iota((64, 64), 1)
    gain = jnp.sum(jnp.where(diagonal, gain_ref[...], 0.0), axis=1, keepdims=True)
    loads[0].wait()
    loads[1].wait()

    def scale(e, carry):
        for ref in (gate_own, up_own):
            ref[e] = (ref[e].astype(F32) * gain).astype(BF16)
        return carry

    lax.fori_loop(0, EXPERTS, scale, 0)

    pl.semaphore_wait(barrier, 15)

    def send_gu(k, carry):
        z2, x2 = peer(k)
        e = (z2 % 4) * 4 + x2
        remote(gate_own.at[e], gate_in.at[me], gu_send.at[0], gu_recv.at[0], plane(z2, x2)).start()
        remote(up_own.at[e], up_in.at[me], gu_send.at[1], gu_recv.at[1], plane(z2, x2)).start()
        return carry

    lax.fori_loop(4, EARLY, send_gu, 0)
    lax.fori_loop(1, 4, send_gu, 0)

    def hail(n):
        for side, step in ((0, 1), (1, 7)):
            pl.semaphore_signal(
                wave_sem.at[n, side], inc=1, device_id=plane((z + step) % 8, x), device_id_type=MESH
            )

    def heard(n):
        for side in range(2):
            pl.semaphore_wait(wave_sem.at[n, side], 1)

    hail(0)

    loads[4].wait()
    loads[5].wait()
    r0, r1 = routes_ref[0:1, :].astype(F32), routes_ref[1:2, :].astype(F32)
    names = iota((EXPERTS, TOK), 0).astype(F32)
    named = jnp.where((names == r0) | (names == r1), 1.0, 0.0)
    earlier = jnp.where(iota((TOK, TOK), 0) < iota((TOK, TOK), 1), 1.0, 0.0).astype(BF16)
    ranks = jnp.dot(named.astype(BF16), earlier, preferred_element_type=F32)
    for k, name in enumerate((r0, r1)):
        rank = jnp.sum(jnp.where(names == name, ranks, 0.0), axis=0, keepdims=True)
        dest[k : k + 1, :] = name * CAP + rank
        late = jnp.where(rank >= CAP // 2, float(PACKED - CAP // 2), 0.0)
        dest[2 + k : 3 + k, :] = name * (CAP // 2) + rank + late

    loads[2].wait()
    loads[3].wait()

    def norm(b, carry):
        at = pl.ds(pl.multiple_of(b * 64, 64), 64)
        full = tok[at, :].astype(F32)
        inverse = lax.rsqrt(jnp.mean(full * full, axis=-1, keepdims=True) + EPSILON)
        normed[at, :] = (mine[at, :].astype(F32) * inverse).astype(BF16)
        return carry

    lax.fori_loop(0, TOK // 64, norm, 0)
    heard(0)
    hail(1)

    def pick(e, carry):
        slot = (iota((CAP, TOK), 0) + e * CAP).astype(F32)
        hits = jnp.where((slot == dest[0:1, :]) | (slot == dest[1:2, :]), 1.0, 0.0).astype(BF16)
        outgoing[e] = jnp.dot(hits, normed[...], preferred_element_type=F32).astype(BF16)
        return carry

    lax.fori_loop(0, EXPERTS, pick, 0)
    heard(1)
    hail(2)

    def slot_at(z2, z1):
        return (z1 - z2 + 2 - z2 % 2 + 16) % 8

    home = slot_at(z, z) * 4 + x

    def block(slot):
        return pl.ds(pl.multiple_of(slot * CAP, CAP), CAP)

    steps = [0, 1, 7, (1 - odd) * 2 + odd * 6]
    tok_self = pltpu.make_async_copy(outgoing.at[fs], rows.at[tp, block(home)], self_sem.at[0])
    tok_self.start()
    for i in range(4):
        for turn in range(4):
            if i + turn:
                z2, x2 = (z + steps[i]) % 8, (x + turn) % 4
                remote(
                    outgoing.at[(z2 % 4) * 4 + x2], rows.at[tp, block(slot_at(z2, z) * 4 + x)],
                    tok_send, tok_recv, plane(z2, x2),
                ).start()

    loads[7].wait()
    selves = [
        pltpu.make_async_copy(gate_own.at[fs], gate_in.at[me], self_sem.at[1]),
        pltpu.make_async_copy(up_own.at[fs], up_in.at[me], self_sem.at[2]),
        pltpu.make_async_copy(down_own.at[fs], down_in.at[me], self_sem.at[3]),
    ]
    for copy in selves:
        copy.start()

    heard(2)
    lax.fori_loop(EARLY, 32, lambda k, carry: send_gu(31 + EARLY - k, carry), 0)

    def band(r):
        return pl.ds(pl.multiple_of(r * DEPTH, DEPTH), DEPTH)

    def send_dn(n, carry):
        r, k = n // 31, 31 - n % 31
        z2, x2 = peer(k)
        remote(
            down_own.at[(z2 % 4) * 4 + x2, band(r)], down_in.at[me, band(r)],
            dn_send, dn_recv.at[r], plane(z2, x2),
        ).start()
        return carry

    lax.fori_loop(0, 31 * ROUNDS, send_dn, 0)

    across = iota((TOK, TOK), 0) == iota((TOK, TOK), 1)

    def upright(row):
        return jnp.sum(jnp.where(across, row, 0.0), axis=1, keepdims=True)

    mine_cols = jnp.concatenate(
        [upright(dest[2:3, :]), upright(dest[3:4, :]), upright(weight_ref[0:1, :]), upright(weight_ref[1:2, :])], axis=1
    )
    for b in range(8):
        cols = mine_cols[b * 64 : (b + 1) * 64]
        slot = iota((64, ROWS), 1).astype(F32)
        cmap[b * 64 : (b + 1) * 64, :] = (
            jnp.where(slot == cols[:, 0:1], cols[:, 2:3], 0.0) + jnp.where(slot == cols[:, 1:2], cols[:, 3:4], 0.0)
        ).astype(BF16)

    tok_self.wait()
    drained(outgoing.at[0:15], tok_recv)
    turns = (1, 3, 2)
    y_copies = [
        remote(rows.at[tp], rows.at[tp], y_send.at[turn - 1], y_recv.at[turn - 1], column((y + turn) % 4, core))
        for turn in turns
    ]
    for copy in y_copies:
        copy.start()
    core_copies = [remote(rows.at[tp], rows.at[tp], core_send.at[0], core_recv.at[0], column(y, 1 - core))]
    core_copies[0].start()
    for turn in turns:
        origin = ((y - turn + 4) % 4) * 2 + core
        drained(rows.at[origin], y_recv.at[turn - 1])
        core_copies.append(
            remote(rows.at[origin], rows.at[origin], core_send.at[turn], core_recv.at[turn], column(y, 1 - core))
        )
        core_copies[-1].start()
    for copy in core_copies:
        copy.wait_recv()

    for copy in selves:
        copy.wait()
    drained(gate_in.at[0:31], gu_recv.at[0])
    drained(up_in.at[0:31], gu_recv.at[1])

    def units(m, carry):
        at = pl.ds(pl.multiple_of(m * 4 * CAP, 4 * CAP), 4 * CAP)
        gate, upper = jnp.zeros((4 * CAP, UNITS), F32), jnp.zeros((4 * CAP, UNITS), F32)
        for j in range(TP):
            lhs = rows[j, at, :]
            gate += jnp.dot(lhs, gate_in[4 * j : 4 * j + 4].reshape(PART, UNITS), preferred_element_type=F32)
            upper += jnp.dot(lhs, up_in[4 * j : 4 * j + 4].reshape(PART, UNITS), preferred_element_type=F32)
        value = (gate / (1.0 + jnp.exp(-gate)) * upper).astype(BF16).reshape(4, 2, CAP // 2, UNITS)
        for half in range(2):
            hidden[half, pl.ds(4 * m, 4)] = value[:, half]
        return carry

    lax.fori_loop(0, EXPERTS // 4, units, 0)

    left = iota((8 * CAP // 2, LANES), 1) < LANES // 2
    pair_copies, ring_copies = [], []

    def half_block(slot):
        return pl.ds(pl.multiple_of(slot * (CAP // 2), CAP // 2), CAP // 2)

    backs = [back.at[r] for r in range(ROUNDS - 1)] + [back_ref]

    def give_back(r):
        home_back = backs[r].at[fs]
        selves.append(pltpu.make_async_copy(result.at[r, half_block(home)], home_back, self_sem.at[4 + r]))
        selves[-1].start()
        homes = [0, 1, 7, (1 - odd) * 6 + odd * 2]
        for i in (3, 1, 2, 0):
            for turn in range(4):
                if i + turn:
                    z1, x1 = (z + homes[i]) % 8, (x + turn) % 4
                    remote(
                        result.at[r, half_block(slot_at(z, z1) * 4 + x1)], home_back,
                        back_send.at[r], back_recv.at[r], plane(z1, x1),
                    ).start()

    def sum_cores(r):
        drained(down_in.at[0:31, 0:DEPTH], dn_recv.at[r])

        def partial(parity, store):
            down = jnp.concatenate(
                [
                    down_in[pl.ds(4 * (2 * k + parity), 4), r * DEPTH : (r + 1) * DEPTH].reshape(4 * DEPTH, UNITS)
                    for k in range(4)
                ],
                axis=0,
            )

            for m in range(2):
                outs = [
                    lax.dot_general(
                        hidden[half, 8 * m : 8 * m + 8].reshape(4 * CAP, UNITS), down, (((1,), (1,)), ((), ())),
                        preferred_element_type=F32,
                    )
                    for half in range(2)
                ]
                for two in range(2):
                    lanes = slice(two * LANES, (two + 1) * LANES)
                    low, high = outs[0][:, lanes], outs[1][:, lanes]
                    at = slice(m * 4 * CAP, (m + 1) * 4 * CAP)
                    store(2 * two, at, jnp.where(left, low, pltpu.roll(high, LANES // 2, 1)))
                    store(2 * two + 1, at, jnp.where(left, pltpu.roll(low, LANES // 2, 1), high))

        def give(y2, at, value):
            pair_out[r, y2, at, :] = value.astype(BF16)

        def keep(y2, at, value):
            own[r, y2, at, :] = value

        partial(1 - core, give)
        for turn in (2, 1, 3, 0):
            y2 = (y + turn) % 4
            pair_copies.append(
                remote(
                    pair_out.at[r, y2], pair_in.at[r, y2], pair_send.at[r, y2], pair_recv.at[r, y2],
                    column(y, 1 - core),
                )
            )
            pair_copies[-1].start()
        partial(core, keep)
        low, high = slice(0, PACKED // 2), slice(PACKED // 2, PACKED)
        sides = ((0, (y + 1) % 4, low, high), (1, (y + 3) % 4, high, low))

        def ring(n, src, dst, device):
            ring_copies.append(remote(src, dst, ring_send.at[r, n], ring_recv.at[r, n], device))
            ring_copies[-1].start()

        for n, turn in enumerate((2, 1, 3, 0)):
            y2 = (y + turn) % 4
            pair_copies[4 * r + n].wait_recv()
            chip[r, y2] = (own[r, y2] + pair_in[r, y2].astype(F32)).astype(BF16)
            if turn == 2:
                for n, near, first, _ in sides:
                    ring(n, chip.at[r, y2, first], relay.at[r, n], column(near, core))
        for n, near, _, second in sides:
            ring(2 + n, chip.at[r, near, second], ring_in.at[r, n, second], column(near, core))
        if r == ROUNDS - 1:
            for before in range(r - 1):
                give_back(before)
        for n, near, first, _ in sides:
            ring_copies[6 * r + n].wait_recv()
            merged[r, n] = (chip[r, near, first].astype(F32) + relay[r, n].astype(F32)).astype(BF16)
            ring(4 + n, merged.at[r, n], ring_in.at[r, n, first], column(near, core))

    def sum_chips(r):
        for copy in ring_copies[6 * r + 2 : 6 * r + 6]:
            copy.wait_recv()
        value = chip[r, y].astype(F32)
        for n in range(2):
            value += ring_in[r, n].astype(F32)
        result[r] = value.astype(BF16)

    def mix(r):
        selves[3 + r].wait()
        drained(back.at[r, 0:15], back_recv.at[r])
        return mix_of(cmap, back[r])

    sum_cores(0)
    for r in range(1, ROUNDS):
        sum_cores(r)
        sum_chips(r - 1)
    give_back(ROUNDS - 2)
    sum_chips(ROUNDS - 1)
    give_back(ROUNDS - 1)
    begun_ref[:, :LANES] = in_lanes(mix(0), mix(1))
    begun_ref[:, LANES:] = mix(2)
    selves[6].wait()
    drained(back_ref.at[0:15], back_recv.at[3])

    drained(outgoing.at[0:15], tok_send)
    drained(gate_in.at[0:31], gu_send.at[0])
    drained(up_in.at[0:31], gu_send.at[1])
    drained(down_in.at[0:31], dn_send)
    for r in range(ROUNDS):
        drained(backs[r].at[0:15], back_send.at[r])
    for copy in y_copies + core_copies + pair_copies + ring_copies:
        copy.wait_send()


def body(tokens, routes, route_weight, gain, w_gate, w_up, w_down):
    anywhere = pl.BlockSpec(memory_space=pl.ANY)
    vmem = pl.BlockSpec(memory_space=pltpu.VMEM)
    weights = pltpu.VMEM((SOURCES, 64, UNITS), BF16)
    dma = pltpu.SemaphoreType.DMA
    held = pl.pallas_call(
        kernel,
        out_shape=(
            weights, weights, weights,
            pltpu.VMEM((TOK, ROWS), BF16),
            pltpu.VMEM((TOK, 2 * LANES), F32),
            pltpu.VMEM((EXPERTS, CAP // 2, LANES), BF16),
        ),
        in_specs=[anywhere] * 7,
        out_specs=(vmem,) * 6,
        scratch_shapes=[
            pltpu.VMEM((2, TOK), jnp.int32),
            pltpu.VMEM((2, TOK), F32),
            pltpu.VMEM((1, D // SOURCES), F32),
            pltpu.VMEM((TOK, D), BF16),
            pltpu.VMEM((TOK, PART), BF16),
            pltpu.VMEM((TOK, PART), BF16),
            pltpu.VMEM((4, TOK), F32),
            pltpu.VMEM((EXPERTS, 64, UNITS), BF16),
            pltpu.VMEM((EXPERTS, 64, UNITS), BF16),
            pltpu.VMEM((EXPERTS, 64, UNITS), BF16),
            pltpu.VMEM((EXPERTS, CAP, PART), BF16),
            pltpu.VMEM((TP, ROWS, PART), BF16),
            pltpu.VMEM((2, EXPERTS, CAP // 2, UNITS), BF16),
            pltpu.VMEM((ROUNDS, 4, PACKED, LANES), BF16),
            pltpu.VMEM((ROUNDS, 4, PACKED, LANES), BF16),
            pltpu.VMEM((ROUNDS, 4, PACKED, LANES), F32),
            pltpu.VMEM((ROUNDS, 4, PACKED, LANES), BF16),
            pltpu.VMEM((ROUNDS, 2, PACKED // 2, LANES), BF16),
            pltpu.VMEM((ROUNDS, 2, PACKED // 2, LANES), BF16),
            pltpu.VMEM((ROUNDS, 2, PACKED, LANES), BF16),
            pltpu.VMEM((ROUNDS, PACKED, LANES), BF16),
            pltpu.VMEM((ROUNDS - 1, EXPERTS, CAP // 2, LANES), BF16),
            dma((8,)),
            pltpu.SemaphoreType.REGULAR((3, 2)),
            dma((8,)),
            dma((2,)), dma((2,)),
            dma, dma((ROUNDS,)),
            dma, dma,
            dma((3,)), dma((3,)),
            dma((4,)), dma((4,)),
            dma((ROUNDS, 4)), dma((ROUNDS, 4)),
            dma((ROUNDS, 6)), dma((ROUNDS, 6)),
            dma((ROUNDS,)), dma((ROUNDS,)),
        ],
        compiler_params=pltpu.CompilerParams(
            collective_id=0, has_side_effects=True, vmem_limit_bytes=48 * 1024 * 1024
        ),
    )(tokens, routes.T, route_weight.T, gain.reshape(1, -1), w_gate, w_up, w_down)
    placed = jax.ShapeDtypeStruct((SOURCES, 64, UNITS), BF16)
    gate_out, up_out, down_out, mixed = pl.pallas_call(
        finish,
        out_shape=(placed, placed, placed, jax.ShapeDtypeStruct((TOK, PART), BF16)),
        in_specs=[vmem] * 6,
        out_specs=(anywhere,) * 4,
        scratch_shapes=[pltpu.VMEM((TOK, PART), BF16), dma((4,))],
        compiler_params=pltpu.CompilerParams(vmem_limit_bytes=16 * 1024 * 1024),
    )(*held)
    return tuple(w.reshape(1, D, UNITS) for w in (gate_out, up_out, down_out)) + (mixed,)


def solution(mesh):
    rows = ("gr", "fs")
    weights = P(None, rows, "tp")
    placed = P("fs", None, "tp")
    return jax.shard_map(
        body,
        mesh=mesh,
        in_specs=(P(rows, None), P(rows, None), P(rows, None), P(rows), weights, weights, weights),
        out_specs=(placed, placed, placed, P(rows, "tp")),
        check_vma=False,
    )
```
